32 devices in a mesh: fs: 16 (over z, y, x), tp: 2 (over core).
Axes of the slice: x: 2, y: 2, z: 4, core: 2. Of those that a mesh axis runs over, the one named last changes fastest.
Arguments:
- tokens: bfloat16 [4096, 2048], P('fs'), may hold values from -6 to 6
- mix_gain: float32 [2048], replicated, may hold values from 0.1 to 1.9
- glu_value: bfloat16 [2048, 2048], P('fs', 'tp'), may hold values from -0.125 to 0.125
- glu_gate: bfloat16 [2048, 2048], P('fs', 'tp'), may hold values from -0.125 to 0.125
- conv_taps: float32 [31, 2048], P(None, 'tp'), may hold values from -2.2 to 2.2, as said below
- chan_gain: float32 [2048], P('tp'), may hold values from 0.1 to 1.9
- mix_out: bfloat16 [2048, 2048], P('tp', 'fs'), may hold values from -0.125 to 0.125
- mlp_gain: float32 [2048], replicated, may hold values from 0.1 to 1.9
- up_weight: bfloat16 [2048, 8192], P('fs', 'tp'), may hold values from -0.125 to 0.125
- down_weight: bfloat16 [8192, 2048], P('tp', 'fs'), may hold values from -0.0625 to 0.0625
Outputs:
- result: bfloat16 [4096, 2048], P('fs')
The draws below stay inside these ranges and needn't reach their ends.
Inputs may be any that keep to these rules, and one draw needn't show every extreme that they name: `conv_taps`: independent entries scaled by fan-in; channels fall into 16 groups of different scale.
All inputs are finite; a program needn't handle non-finite values.
Results may differ from the reference program's by a relative error of at most 0.018.
Values may be sent and summed in bfloat16 or wider, within the bound.
A program may use at most 128 MiB of HBM per device.

```python
import jax
import jax.numpy as jnp
from jax import lax

D = 2048
C = 2048
FF = 8192
WIDTH = 31
LEN = 128
TOKENS = 4096
N_TP = 2


def draw_conv_taps(key, part):
    first, second = jax.random.split(key)
    raw_taps = jnp.clip(jax.random.normal(first, (WIDTH, C), jnp.float32), -4.0, 4.0)
    levels = jnp.exp(jax.random.uniform(second, (16,), jnp.float32, jnp.log(0.3), jnp.log(3.0)))
    return raw_taps * WIDTH ** (-0.5) * jnp.repeat(levels, C // 16)


def block_scale(own_key, dims, shards, smallest, largest):
    def one(position, shards_of):
        heights = jax.random.uniform(jax.random.fold_in(jax.random.fold_in(own_key, 6), position), (shards_of,), jnp.float32, smallest / len(shards), largest / len(shards))
        return jnp.repeat(jnp.exp(heights), dims[position] // shards_of).reshape((-1,) + (1,) * (len(dims) - position - 1))

    level = one(*shards[0])
    for cut in shards[1:]:
        level = level * one(*cut)
    return level


def centred(stream_key, dims, scale, limit, shards=(), held_as=jnp.bfloat16):
    values = jax.random.normal(stream_key, dims, jnp.float32) * scale
    if len(shards) > 0:
        values = block_scale(stream_key, dims, shards, -0.22, 0.18) * values
    return jnp.clip(values, min=-limit, max=limit).astype(held_as)


def setup_inputs(seed: int = 0) -> dict:
    streams_of = jax.random.split(jax.random.key(seed), 11)
    tokens = centred(streams_of[0], (TOKENS, D), 1.0, 6.0, ((0, 16),))
    mix_gain = jnp.clip(1.0 + 0.18 * jax.random.normal(streams_of[1], (D,), jnp.float32), 0.1, 1.9)
    glu_value = centred(streams_of[2], (D, C), D ** -0.5, 0.125, ((0, 16), (1, 2)))
    glu_gate = centred(streams_of[3], (D, C), D ** -0.5, 0.125, ((0, 16), (1, 2)))
    conv_taps = draw_conv_taps(jax.random.fold_in(streams_of[10], 71), 0)
    chan_gain = jnp.clip(1.0 + 0.18 * jax.random.normal(streams_of[5], (C,), jnp.float32), 0.1, 1.9)
    mix_out = centred(streams_of[6], (C, D), C ** -0.5, 0.125, ((0, 2), (1, 16)))
    mlp_gain = jnp.clip(1.0 + 0.18 * jax.random.normal(streams_of[7], (D,), jnp.float32), 0.1, 1.9)
    up_weight = centred(streams_of[8], (D, FF), D ** -0.5, 0.125, ((0, 16), (1, 2)))
    down_weight = centred(streams_of[9], (FF, D), FF ** -0.5, 0.0625, ((0, 2), (1, 16)))
    return {"tokens": tokens, "mix_gain": mix_gain, "glu_value": glu_value, "glu_gate": glu_gate, "conv_taps": conv_taps, "chan_gain": chan_gain, "mix_out": mix_out, "mlp_gain": mlp_gain, "up_weight": up_weight, "down_weight": down_weight}


norm_floor = 0.05

def rms_scale(stream, gain):
    return stream * lax.rsqrt(lax.optimization_barrier(jnp.mean(stream * stream, axis=-1, keepdims=True)) + norm_floor) * gain

def bf16_round(value):
    return lax.optimization_barrier(value.astype(jnp.bfloat16)).astype(jnp.float32)

def depthwise(glu, conv_taps):
    seqs = glu.shape[0] // LEN
    blocks = glu.reshape(seqs, LEN, glu.shape[1]).astype(jnp.float32)
    reach = conv_taps.shape[0] // 2
    padded = jnp.pad(blocks, ((0, 0), (reach, reach), (0, 0)))
    total = jnp.zeros_like(blocks)
    for offset in range(conv_taps.shape[0]):
        total = total + padded[:, offset:offset + LEN] * conv_taps[offset]
    return total.reshape(glu.shape)

def shard_sum(left, right):
    block = left.shape[1] // N_TP
    total = jnp.zeros((left.shape[0], right.shape[1]), jnp.float32)
    for shard in range(N_TP):
        partial_term = jnp.dot(left[:, shard * block:(shard + 1) * block], right[shard * block:(shard + 1) * block], preferred_element_type=jnp.float32)
        total = total + bf16_round(partial_term)
    return total.astype(jnp.bfloat16)

def reference(tokens, mix_gain, glu_value, glu_gate, conv_taps, chan_gain, mix_out, mlp_gain, up_weight, down_weight):
    stream = tokens.astype(jnp.float32)
    normed = rms_scale(stream, mix_gain).astype(jnp.bfloat16)
    values = jnp.dot(normed, glu_value, preferred_element_type=jnp.float32)
    gating = jnp.dot(normed, glu_gate, preferred_element_type=jnp.float32)
    glu = (values * jax.nn.sigmoid(gating)).astype(jnp.bfloat16)
    convolved = depthwise(glu, conv_taps)
    centre = lax.optimization_barrier(jnp.mean(convolved, axis=-1, keepdims=True))
    spread = lax.optimization_barrier(jnp.mean(convolved * convolved, axis=-1, keepdims=True)) - centre * centre
    hidden = jax.nn.silu((convolved - centre) * lax.rsqrt(spread + norm_floor) * chan_gain).astype(jnp.bfloat16)
    mixed = shard_sum(hidden, mix_out)
    resid = stream + mixed.astype(jnp.float32)
    normed_mlp = rms_scale(resid, mlp_gain).astype(jnp.bfloat16)
    active = jnp.square(jax.nn.relu(jnp.dot(normed_mlp, up_weight, preferred_element_type=jnp.float32))).astype(jnp.bfloat16)
    feed = shard_sum(active, down_weight)
    return (resid + feed.astype(jnp.float32)).astype(jnp.bfloat16)
```

```python
import jax
import jax.numpy as jnp
from jax import lax
from jax.sharding import PartitionSpec as P

C = 2048
LEN = 128


norm_floor = 0.05


def rms_scale(stream, gain):
    return stream * lax.rsqrt(jnp.mean(stream * stream, axis=-1, keepdims=True) + norm_floor) * gain


def bf16_round(value):
    return lax.optimization_barrier(value.astype(jnp.bfloat16)).astype(jnp.float32)


def depthwise(glu, conv_taps):
    seqs = glu.shape[0] // LEN
    blocks = glu.reshape(seqs, LEN, glu.shape[1]).astype(jnp.float32)
    reach = conv_taps.shape[0] // 2
    padded = jnp.pad(blocks, ((0, 0), (reach, reach), (0, 0)))
    total = jnp.zeros_like(blocks)
    for offset in range(conv_taps.shape[0]):
        total = total + padded[:, offset : offset + LEN] * conv_taps[offset]
    return total.reshape(glu.shape)


def swap_then_gather(weight, inner, outer, split, join):
    own = lax.all_to_all(
        weight, "fs", split_axis=split, concat_axis=join, axis_index_groups=inner, tiled=True
    )
    return lax.all_gather(own, "fs", axis=join, axis_index_groups=outer, tiled=True)


def shared_sum(partial, inner, tp):
    part = lax.all_to_all(
        partial, "fs", split_axis=0, concat_axis=0, axis_index_groups=inner, tiled=True
    )
    group = len(inner[0])
    rows = partial.shape[0] // group
    part = part.reshape(group, tp, rows // tp, -1).transpose(1, 0, 2, 3)
    part = lax.all_to_all(part, "tp", split_axis=0, concat_axis=0, tiled=True)
    return bf16_round(jnp.sum(part.astype(jnp.float32), axis=(0, 1)))


def per_device(
    tokens,
    mix_gain,
    glu_value,
    glu_gate,
    conv_taps,
    chan_gain,
    mix_out,
    mlp_gain,
    up_weight,
    down_weight,
):
    fs, tp = lax.axis_size("fs"), lax.axis_size("tp")
    group = 4 if fs % 4 == 0 else 1
    inner = [[o * group + i for i in range(group)] for o in range(fs // group)]
    outer = [[o * group + i for o in range(fs // group)] for i in range(group)]
    place = lax.rem(lax.axis_index("fs"), group)

    value_w = swap_then_gather(glu_value, inner, outer, 1, 0)
    gate_w = swap_then_gather(glu_gate, inner, outer, 1, 0)
    mix_w = swap_then_gather(mix_out, inner, outer, 0, 1)
    up_w = swap_then_gather(up_weight, inner, outer, 1, 0)
    down_w = swap_then_gather(down_weight, inner, outer, 0, 1)

    stream = tokens.astype(jnp.float32)
    normed = rms_scale(stream, mix_gain).astype(jnp.bfloat16)
    normed = lax.all_gather(normed, "fs", axis=0, axis_index_groups=inner, tiled=True)
    values = jnp.dot(normed, value_w, preferred_element_type=jnp.float32)
    gating = jnp.dot(normed, gate_w, preferred_element_type=jnp.float32)
    glu = (values * jax.nn.sigmoid(gating)).astype(jnp.bfloat16)
    channels = value_w.shape[1]
    taps = lax.dynamic_slice_in_dim(conv_taps, place * channels, channels, 1)
    gain = lax.dynamic_slice_in_dim(chan_gain, place * channels, channels, 0)
    convolved = depthwise(glu, taps)
    both = jnp.stack(
        (jnp.sum(convolved, axis=-1), jnp.sum(convolved * convolved, axis=-1))
    )
    both = jnp.sum(lax.all_gather(both, "fs", axis=0, axis_index_groups=inner), axis=0)
    both = lax.psum(both, "tp")
    centre = (both[0] / C)[:, None]
    spread = (both[1] / C)[:, None] - centre * centre
    hidden = jax.nn.silu((convolved - centre) * lax.rsqrt(spread + norm_floor) * gain).astype(
        jnp.bfloat16
    )
    mixed = shared_sum(
        jnp.dot(hidden, mix_w, preferred_element_type=jnp.float32).astype(jnp.bfloat16), inner, tp
    )
    own_rows = stream.shape[0] // tp
    own_stream = lax.dynamic_slice_in_dim(stream, lax.axis_index("tp") * own_rows, own_rows, 0)
    resid = own_stream + mixed
    normed_mlp = rms_scale(resid, mlp_gain).astype(jnp.bfloat16)
    normed_mlp = lax.all_gather(normed_mlp, "fs", axis=0, axis_index_groups=inner)
    normed_mlp = lax.all_gather(normed_mlp, "tp", axis=1).reshape(-1, normed.shape[1])
    active = jnp.square(
        jax.nn.relu(jnp.dot(normed_mlp, up_w, preferred_element_type=jnp.float32))
    ).astype(jnp.bfloat16)
    feed = shared_sum(
        jnp.dot(active, down_w, preferred_element_type=jnp.float32).astype(jnp.bfloat16), inner, tp
    )
    finished = (resid + feed).astype(jnp.bfloat16)
    return lax.all_gather(finished, "tp", axis=0, tiled=True)

def solution(mesh):
    in_specs = (
        P("fs", None),
        P(),
        P("fs", "tp"),
        P("fs", "tp"),
        P(None, "tp"),
        P("tp"),
        P("tp", "fs"),
        P(),
        P("fs", "tp"),
        P("tp", "fs"),
    )
    out_specs = P("fs", None)
    return jax.shard_map(
        per_device, mesh=mesh, in_specs=in_specs, out_specs=out_specs, check_vma=False
    )
```

```python
import functools

import jax
import jax.numpy as jnp
from jax import lax
from jax.experimental import pallas as pl
from jax.experimental.pallas import tpu as pltpu
from jax.sharding import PartitionSpec as P

C = 2048
LEN = 128


norm_floor = 0.05


def rms_scale(stream, gain):
    return stream * lax.rsqrt(jnp.mean(stream * stream, axis=-1, keepdims=True) + norm_floor) * gain


def bf16_round(value):
    return lax.optimization_barrier(value.astype(jnp.bfloat16)).astype(jnp.float32)


def depthwise(glu, conv_taps):
    seqs = glu.shape[0] // LEN
    blocks = glu.reshape(seqs, LEN, glu.shape[1]).astype(jnp.float32)
    reach = conv_taps.shape[0] // 2
    padded = jnp.pad(blocks, ((0, 0), (reach, reach), (0, 0)))
    total = jnp.zeros_like(blocks)
    for offset in range(conv_taps.shape[0]):
        total = total + padded[:, offset : offset + LEN] * conv_taps[offset]
    return total.reshape(glu.shape)


def swap_then_gather(weight, inner, outer, split, join):
    own = lax.all_to_all(
        weight, "fs", split_axis=split, concat_axis=join, axis_index_groups=inner, tiled=True
    )
    return lax.all_gather(own, "fs", axis=join, axis_index_groups=outer, tiled=True)


def shared_sum(partial, inner, tp):
    part = lax.all_to_all(
        partial, "fs", split_axis=0, concat_axis=0, axis_index_groups=inner, tiled=True
    )
    group = len(inner[0])
    rows = partial.shape[0] // group
    part = part.reshape(group, tp, rows // tp, -1).transpose(1, 0, 2, 3)
    part = lax.all_to_all(part, "tp", split_axis=0, concat_axis=0, tiled=True)
    return bf16_round(jnp.sum(part.astype(jnp.float32), axis=(0, 1)))


def plain_device(
    tokens,
    mix_gain,
    glu_value,
    glu_gate,
    conv_taps,
    chan_gain,
    mix_out,
    mlp_gain,
    up_weight,
    down_weight,
):
    fs, tp = lax.axis_size("fs"), lax.axis_size("tp")
    group = 4 if fs % 4 == 0 else 1
    inner = [[o * group + i for i in range(group)] for o in range(fs // group)]
    outer = [[o * group + i for o in range(fs // group)] for i in range(group)]
    place = lax.rem(lax.axis_index("fs"), group)

    value_w = swap_then_gather(glu_value, inner, outer, 1, 0)
    gate_w = swap_then_gather(glu_gate, inner, outer, 1, 0)
    mix_w = swap_then_gather(mix_out, inner, outer, 0, 1)
    up_w = swap_then_gather(up_weight, inner, outer, 1, 0)
    down_w = swap_then_gather(down_weight, inner, outer, 0, 1)

    stream = tokens.astype(jnp.float32)
    normed = rms_scale(stream, mix_gain).astype(jnp.bfloat16)
    normed = lax.all_gather(normed, "fs", axis=0, axis_index_groups=inner, tiled=True)
    values = jnp.dot(normed, value_w, preferred_element_type=jnp.float32)
    gating = jnp.dot(normed, gate_w, preferred_element_type=jnp.float32)
    glu = (values * jax.nn.sigmoid(gating)).astype(jnp.bfloat16)
    channels = value_w.shape[1]
    taps = lax.dynamic_slice_in_dim(conv_taps, place * channels, channels, 1)
    gain = lax.dynamic_slice_in_dim(chan_gain, place * channels, channels, 0)
    convolved = depthwise(glu, taps)
    both = jnp.stack(
        (jnp.sum(convolved, axis=-1), jnp.sum(convolved * convolved, axis=-1))
    )
    both = jnp.sum(lax.all_gather(both, "fs", axis=0, axis_index_groups=inner), axis=0)
    both = lax.psum(both, "tp")
    centre = (both[0] / C)[:, None]
    spread = (both[1] / C)[:, None] - centre * centre
    hidden = jax.nn.silu((convolved - centre) * lax.rsqrt(spread + norm_floor) * gain).astype(
        jnp.bfloat16
    )
    mixed = shared_sum(
        jnp.dot(hidden, mix_w, preferred_element_type=jnp.float32).astype(jnp.bfloat16), inner, tp
    )
    own_rows = stream.shape[0] // tp
    own_stream = lax.dynamic_slice_in_dim(stream, lax.axis_index("tp") * own_rows, own_rows, 0)
    resid = own_stream + mixed
    normed_mlp = rms_scale(resid, mlp_gain).astype(jnp.bfloat16)
    normed_mlp = lax.all_gather(normed_mlp, "fs", axis=0, axis_index_groups=inner)
    normed_mlp = lax.all_gather(normed_mlp, "tp", axis=1).reshape(-1, normed.shape[1])
    active = jnp.square(
        jax.nn.relu(jnp.dot(normed_mlp, up_w, preferred_element_type=jnp.float32))
    ).astype(jnp.bfloat16)
    feed = shared_sum(
        jnp.dot(active, down_w, preferred_element_type=jnp.float32).astype(jnp.bfloat16), inner, tp
    )
    finished = (resid + feed).astype(jnp.bfloat16)
    return lax.all_gather(finished, "tp", axis=0, tiled=True)

MESH = pl.DeviceIdType.MESH
F32, BF16 = jnp.float32, jnp.bfloat16


def rows_at(start, size):
    return pl.ds(pl.multiple_of(start, 128), size)


def layer_kernel(
    ng, nz,
    tok, mixg, gv, gg, taps, chg, mo, mlpg, up, dn,
    out,
    fgv, fgg, fmo, fup, fdn,
    tok_all, nrm, pad, cv, hid, st, st_all,
    acc, resid, nm_all, act, fin,
    sbo1, sbi1, rdo1, rdi1, sbo2, sbi2, rdo2, rdi2,
    ws, wr, lsem, tsem, nsem, ssem, rsem, fsem,
):
    f, t = lax.axis_index("fs"), lax.axis_index("tp")
    p, z = lax.rem(f, ng), lax.div(f, ng)
    sib = 1 - t
    L = tok.shape[0] // 2
    half = ng * L
    width = tok.shape[1]
    chans = fgv.shape[1]
    hidden = fup.shape[1]
    depth = gv.shape[0]
    sends = []

    def chip(dq):
        return lax.rem(p + dq, ng)

    def plane(dz):
        return lax.rem(z + dz, nz)

    def push(src, dst, s_sem, r_sem, device):
        copy = pltpu.make_async_remote_copy(
            src_ref=src, dst_ref=dst, send_sem=s_sem, recv_sem=r_sem,
            device_id=device, device_id_type=MESH,
        )
        copy.start()
        sends.append(copy)

    def arrived(dst, s_sem, r_sem):
        pltpu.make_async_remote_copy(
            src_ref=dst, dst_ref=dst, send_sem=s_sem, recv_sem=r_sem,
            device_id=(f, sib), device_id_type=MESH,
        ).wait_recv()

    barrier = pltpu.get_barrier_semaphore()
    peers = [(z * ng + chip(dq), u) for dq in range(1, ng) for u in (t, sib)]
    peers += [(f, sib)] + [(plane(dz) * ng + p, t) for dz in range(1, nz)]
    for peer in peers:
        pl.semaphore_signal(barrier, inc=1, device_id=peer, device_id_type=MESH)
    pl.semaphore_wait(barrier, len(peers))

    weights = (
        (lambda q: gv.at[:, rows_at(q * chans, chans)], lambda g: fgv.at[rows_at(g * depth, depth), :]),
        (lambda q: gg.at[:, rows_at(q * chans, chans)], lambda g: fgg.at[rows_at(g * depth, depth), :]),
        (lambda q: mo.at[rows_at(q * chans, chans), :], lambda g: fmo.at[:, rows_at(g * depth, depth)]),
        (lambda q: up.at[:, rows_at(q * hidden, hidden)], lambda g: fup.at[rows_at(g * depth, depth), :]),
        (lambda q: dn.at[rows_at(q * hidden, hidden), :], lambda g: fdn.at[:, rows_at(g * depth, depth)]),
    )

    def spread_in_plane(a):
        src, dst = weights[a]
        for dq in range(1, ng):
            push(src(chip(dq)), dst(f), ws.at[a, dq], wr.at[a, ng - dq], (z * ng + chip(dq), t))

    def spread_own(a):
        src, dst = weights[a]
        for dz in range(1, nz):
            push(src(p), dst(f), ws.at[a, dz * ng], wr.at[a, (nz - dz) * ng], (plane(dz) * ng + p, t))

    def forward(a):
        dst = weights[a][1]
        for dq in range(1, ng):
            piece = dst(z * ng + chip(dq))
            arrived(piece, ws.at[a, 0], wr.at[a, dq])
            for dz in range(1, nz):
                push(piece, piece, ws.at[a, dz * ng + dq], wr.at[a, (nz - dz) * ng + dq], (plane(dz) * ng + p, t))

    def whole(a):
        src, dst = weights[a]
        for dz in range(1, nz):
            for dq in range(ng):
                arrived(dst(plane(dz) * ng + chip(dq)), ws.at[a, 0], wr.at[a, dz * ng + dq])
        local(a).wait()

    def local(a):
        src, dst = weights[a]
        return pltpu.make_async_copy(src(p), dst(f), lsem.at[a])

    for a in (0, 1):
        spread_in_plane(a)
    for a in (0, 1):
        spread_own(a)
    for dq in range(1, ng):
        push(
            tok.at[rows_at(t * L, L)], tok_all.at[rows_at(t * half + p * L, L)],
            tsem.at[0, dq], tsem.at[1, ng - dq], (z * ng + chip(dq), t),
        )
    spread_in_plane(2)
    spread_own(2)
    for a in (3, 4):
        spread_in_plane(a)
    for a in range(5):
        local(a).start()

    step = 16

    def norm_rows(load, gain, dst, start):
        def body(i, _):
            value = load(i * step).astype(F32)
            scale = lax.rsqrt(jnp.mean(value * value, axis=-1, keepdims=True) + norm_floor)
            dst[pl.ds(pl.multiple_of(start + i * step, step), step), :] = (
                value * scale * gain[...]
            ).astype(BF16)
            return 0

        lax.fori_loop(0, L // step, body, 0)

    def from_ref(ref, base):
        return lambda i: ref[pl.ds(pl.multiple_of(base + i, step), step), :]

    for u in range(2):
        norm_rows(from_ref(tok, u * L), mixg, nrm, u * half + p * L)
    for a in (0, 1):
        forward(a)
    for dq in range(1, ng):
        block = tok_all.at[rows_at(t * half + chip(dq) * L, L)]
        arrived(block, tsem.at[0, 0], tsem.at[1, dq])
        push(block, block, tsem.at[2, dq], tsem.at[3, dq], (f, sib))
        norm_rows(from_ref(tok_all, t * half + chip(dq) * L), mixg, nrm, t * half + chip(dq) * L)
    forward(2)
    for a in (3, 4):
        spread_own(a)
    for dq in range(1, ng):
        start = sib * half + chip(dq) * L
        arrived(tok_all.at[rows_at(start, L)], tsem.at[0, 0], tsem.at[3, dq])
        norm_rows(from_ref(tok_all, start), mixg, nrm, start)

    whole(0)
    whole(1)
    pad[...] = jnp.zeros_like(pad)
    st[...] = jnp.zeros_like(st)
    taps_n = taps.shape[0]
    reach = taps_n // 2
    lead = (reach + 7) // 8 * 8
    own_cols = p * chans
    eye = lax.broadcasted_iota(jnp.int32, (L, L), 0) == lax.broadcasted_iota(jnp.int32, (L, L), 1)

    def conv_block(b, _):
        rows = rows_at(b * L, L)
        left = nrm[rows, :]
        values = jnp.dot(left, fgv[...], preferred_element_type=F32)
        gating = jnp.dot(left, fgg[...], preferred_element_type=F32)
        glu = (values * jax.nn.sigmoid(gating)).astype(BF16).astype(F32)
        pad[pl.ds(lead, L), :] = glu
        sums = jnp.zeros((L, 1), F32)
        squares = jnp.zeros((L, 1), F32)
        for c in range(chans // 128):
            total = jnp.zeros((L, 128), F32)
            for j in range(taps_n):
                tap = taps[pl.ds(j, 1), rows_at(own_cols + c * 128, 128)]
                total = total + pad[pl.ds(lead - reach + j, L), pl.ds(c * 128, 128)] * tap
            cv[rows, pl.ds(c * 128, 128)] = total
            sums = sums + jnp.sum(total, axis=1, keepdims=True)
            squares = squares + jnp.sum(total * total, axis=1, keepdims=True)
        st[b, pl.ds(0, 1), :] = jnp.sum(jnp.where(eye, sums, 0.0), axis=0, keepdims=True)
        st[b, pl.ds(1, 1), :] = jnp.sum(jnp.where(eye, squares, 0.0), axis=0, keepdims=True)
        return 0

    lax.fori_loop(0, 2 * ng, conv_block, 0)

    slots = [(dq, du) for dq in range(ng) for du in range(2) if (dq, du) != (0, 0)]
    for dq, du in slots:
        push(
            st, st_all.at[(ng - dq) % ng * 2 + du],
            ssem.at[0, dq * 2 + du], ssem.at[1, (ng - dq) % ng * 2 + du],
            (z * ng + chip(dq), t if du == 0 else sib),
        )
    forward(3)
    for dq, du in slots:
        arrived(st_all.at[dq * 2 + du], ssem.at[0, 0], ssem.at[1, dq * 2 + du])

    def hidden_block(b, _):
        rows = rows_at(b * L, L)
        total = st[b]
        for dq, du in slots:
            total = total + st_all[dq * 2 + du, b]
        count = chans * ng * 2
        sums = jnp.sum(jnp.where(eye, total[0:1, :], 0.0), axis=1, keepdims=True)
        squares = jnp.sum(jnp.where(eye, total[1:2, :], 0.0), axis=1, keepdims=True)
        centre = sums / count
        spread = squares / count - centre * centre
        value = (cv[rows, :] - centre) * lax.rsqrt(spread + norm_floor)
        value = value * chg[:, rows_at(own_cols, chans)]
        hid[rows, :] = (value * jax.nn.sigmoid(value)).astype(BF16)
        return 0

    lax.fori_loop(0, 2 * ng, hidden_block, 0)

    cols = 512

    def reduce_rows(left, right, sbo, sbi, rdo, rdi, k):
        def theirs(n, _):
            at = rows_at(n * cols, cols)
            sbo[:, at] = jnp.dot(
                left[rows_at(sib * half, half), :], right[:, at], preferred_element_type=F32
            ).astype(BF16)
            return 0

        lax.fori_loop(0, width // cols, theirs, 0)
        push(sbo, sbi, rsem.at[k, 0], rsem.at[k, 1], (f, sib))

        def mine(n, _):
            at = rows_at(n * cols, cols)
            acc[:, at] = jnp.dot(
                left[rows_at(t * half, half), :], right[:, at], preferred_element_type=F32
            )
            return 0

        lax.fori_loop(0, width // cols, mine, 0)
        arrived(sbi, rsem.at[k, 0], rsem.at[k, 1])
        for dq in range(1, ng):
            base = chip(dq) * L

            def add(i, _):
                at = pl.ds(pl.multiple_of(base + i * step, step), step)
                rdo[at, :] = (acc[at, :] + sbi[at, :].astype(F32)).astype(BF16)
                return 0

            lax.fori_loop(0, L // step, add, 0)
            push(
                rdo.at[rows_at(base, L)], rdi.at[ng - dq - 1],
                rsem.at[k, 2 * dq], rsem.at[k, 2 * (ng - dq) + 1], (z * ng + chip(dq), t),
            )

    def reduced(sbi, rdi, i):
        at = pl.ds(pl.multiple_of(p * L + i * step, step), step)
        total = acc[at, :] + sbi[at, :].astype(F32)
        for dq in range(1, ng):
            total = total + rdi[dq - 1, pl.ds(pl.multiple_of(i * step, step), step), :].astype(F32)
        return total.astype(BF16).astype(F32)

    def wait_reduced(rdi, k):
        for dq in range(1, ng):
            arrived(rdi.at[dq - 1], rsem.at[k, 0], rsem.at[k, 2 * dq + 1])

    whole(2)
    reduce_rows(hid, fmo, sbo1, sbi1, rdo1, rdi1, 0)
    forward(4)
    wait_reduced(rdi1, 0)

    def resid_rows(i, _):
        at = pl.ds(pl.multiple_of(i * step, step), step)
        own = tok[pl.ds(pl.multiple_of(t * L + i * step, step), step), :].astype(F32)
        value = own + reduced(sbi1, rdi1, i)
        resid[at, :] = value
        scale = lax.rsqrt(jnp.mean(value * value, axis=-1, keepdims=True) + norm_floor)
        nm_all[pl.ds(pl.multiple_of(t * half + p * L + i * step, step), step), :] = (
            value * scale * mlpg[...]
        ).astype(BF16)
        return 0

    lax.fori_loop(0, L // step, resid_rows, 0)
    mine = nm_all.at[rows_at(t * half + p * L, L)]
    for dq in range(1, ng):
        push(mine, mine, nsem.at[0, dq], nsem.at[1, ng - dq], (z * ng + chip(dq), t))
    push(mine, mine, nsem.at[2, 0], nsem.at[3, 0], (f, sib))
    for dq in range(1, ng):
        block = nm_all.at[rows_at(t * half + chip(dq) * L, L)]
        arrived(block, nsem.at[0, 0], nsem.at[1, dq])
        push(block, block, nsem.at[2, dq], nsem.at[3, dq], (f, sib))

    whole(3)

    def up_half(u):
        def body(n, _):
            at = rows_at(n * 256, 256)
            value = jnp.dot(
                nm_all[rows_at(u * half, half), :], fup[:, at], preferred_element_type=F32
            )
            value = jnp.maximum(value, 0.0)
            act[rows_at(u * half, half), at] = (value * value).astype(BF16)
            return 0

        lax.fori_loop(0, hidden // 256, body, 0)

    up_half(t)
    for dq in range(ng):
        arrived(nm_all.at[rows_at(sib * half + chip(dq) * L, L)], nsem.at[0, 0], nsem.at[3, dq])
    up_half(sib)
    whole(4)
    reduce_rows(act, fdn, sbo2, sbi2, rdo2, rdi2, 1)
    wait_reduced(rdi2, 1)

    def finish_rows(i, _):
        at = pl.ds(pl.multiple_of(i * step, step), step)
        value = (resid[at, :] + reduced(sbi2, rdi2, i)).astype(BF16)
        fin[0, at, :] = value
        out[pl.ds(pl.multiple_of(t * L + i * step, step), step), :] = value
        return 0

    lax.fori_loop(0, L // step, finish_rows, 0)
    push(fin.at[0], fin.at[1], fsem.at[0], fsem.at[1], (f, sib))
    arrived(fin.at[1], fsem.at[0], fsem.at[1])

    def copy_rows(i, _):
        at = pl.ds(pl.multiple_of(i * step, step), step)
        out[pl.ds(pl.multiple_of(sib * L + i * step, step), step), :] = fin[1, at, :]
        return 0

    lax.fori_loop(0, L // step, copy_rows, 0)
    for copy in sends:
        copy.wait_send()


def fused_device(ng, nz, tokens, mix_gain, glu_value, glu_gate, conv_taps, chan_gain, mix_out, mlp_gain, up_weight, down_weight):
    rows, width = tokens.shape
    fs = ng * nz
    L = rows // 2
    half = ng * L
    chans = glu_value.shape[1] // ng
    hidden = up_weight.shape[1] // ng
    depth = glu_value.shape[0]
    blocks = 2 * ng
    vm = pltpu.VMEM
    dma = pltpu.SemaphoreType.DMA
    reduce_bufs = [
        vm((half, width), BF16), vm((half, width), BF16), vm((half, width), BF16),
        vm((ng - 1, L, width), BF16),
    ]
    scratch = [
        vm((fs * depth, chans), BF16), vm((fs * depth, chans), BF16), vm((chans, width), BF16),
        vm((fs * depth, hidden), BF16), vm((hidden, width), BF16),
        vm((2 * half, width), BF16), vm((2 * half, width), BF16),
        vm((L + 32, chans), F32), vm((2 * half, chans), F32), vm((2 * half, chans), BF16),
        vm((blocks, 8, L), F32), vm((blocks, blocks, 8, L), F32),
        vm((half, width), F32), vm((L, width), F32), vm((2 * half, width), BF16),
        vm((2 * half, hidden), BF16), vm((2, L, width), BF16),
        *reduce_bufs, *reduce_bufs,
        dma((5, fs)), dma((5, fs)), dma((5,)), dma((4, ng)), dma((4, ng)),
        dma((2, blocks)), dma((2, 2 * ng)), dma((2,)),
    ]
    return pl.pallas_call(
        functools.partial(layer_kernel, ng, nz),
        out_shape=jax.ShapeDtypeStruct((rows, width), BF16),
        in_specs=[pl.BlockSpec(memory_space=vm)] * 10,
        out_specs=pl.BlockSpec(memory_space=vm),
        scratch_shapes=scratch,
        compiler_params=pltpu.CompilerParams(
            collective_id=0, has_side_effects=True, vmem_limit_bytes=60 * 1024 * 1024
        ),
    )(
        tokens, mix_gain[None], glu_value, glu_gate, conv_taps, chan_gain[None], mix_out,
        mlp_gain[None], up_weight, down_weight,
    )


def per_device(*args):
    tokens, glu_value, conv_taps = args[0], args[2], args[4]
    fs, tp = lax.axis_size("fs"), lax.axis_size("tp")
    group = 4
    fits = (
        tp == 2
        and fs % group == 0
        and fs > group
        and tokens.shape[0] == 2 * LEN
        and glu_value.shape[0] % 128 == 0
        and conv_taps.shape[1] % (group * 128) == 0
        and conv_taps.shape[0] <= 31
    )
    if fits:
        return fused_device(group, fs // group, *args)
    return plain_device(*args)


def solution(mesh):
    in_specs = (
        P("fs", None),
        P(),
        P("fs", "tp"),
        P("fs", "tp"),
        P(None, "tp"),
        P("tp"),
        P("tp", "fs"),
        P(),
        P("fs", "tp"),
        P("tp", "fs"),
    )
    out_specs = P("fs", None)
    return jax.shard_map(
        per_device, mesh=mesh, in_specs=in_specs, out_specs=out_specs, check_vma=False
    )
```

```python
import functools

import jax
import jax.numpy as jnp
from jax import lax
from jax.experimental import pallas as pl
from jax.experimental.pallas import tpu as pltpu
from jax.sharding import PartitionSpec as P

C = 2048
LEN = 128


norm_floor = 0.05


def rms_scale(stream, gain):
    return stream * lax.rsqrt(jnp.mean(stream * stream, axis=-1, keepdims=True) + norm_floor) * gain


def bf16_round(value):
    return lax.optimization_barrier(value.astype(jnp.bfloat16)).astype(jnp.float32)


def depthwise(glu, conv_taps):
    seqs = glu.shape[0] // LEN
    blocks = glu.reshape(seqs, LEN, glu.shape[1]).astype(jnp.float32)
    reach = conv_taps.shape[0] // 2
    padded = jnp.pad(blocks, ((0, 0), (reach, reach), (0, 0)))
    total = jnp.zeros_like(blocks)
    for offset in range(conv_taps.shape[0]):
        total = total + padded[:, offset : offset + LEN] * conv_taps[offset]
    return total.reshape(glu.shape)


def swap_then_gather(weight, inner, outer, split, join):
    own = lax.all_to_all(
        weight, "fs", split_axis=split, concat_axis=join, axis_index_groups=inner, tiled=True
    )
    return lax.all_gather(own, "fs", axis=join, axis_index_groups=outer, tiled=True)


def shared_sum(partial, inner, tp):
    part = lax.all_to_all(
        partial, "fs", split_axis=0, concat_axis=0, axis_index_groups=inner, tiled=True
    )
    group = len(inner[0])
    rows = partial.shape[0] // group
    part = part.reshape(group, tp, rows // tp, -1).transpose(1, 0, 2, 3)
    part = lax.all_to_all(part, "tp", split_axis=0, concat_axis=0, tiled=True)
    return bf16_round(jnp.sum(part.astype(jnp.float32), axis=(0, 1)))


def plain_device(
    tokens,
    mix_gain,
    glu_value,
    glu_gate,
    conv_taps,
    chan_gain,
    mix_out,
    mlp_gain,
    up_weight,
    down_weight,
):
    fs, tp = lax.axis_size("fs"), lax.axis_size("tp")
    group = 4 if fs % 4 == 0 else 1
    inner = [[o * group + i for i in range(group)] for o in range(fs // group)]
    outer = [[o * group + i for o in range(fs // group)] for i in range(group)]
    place = lax.rem(lax.axis_index("fs"), group)

    value_w = swap_then_gather(glu_value, inner, outer, 1, 0)
    gate_w = swap_then_gather(glu_gate, inner, outer, 1, 0)
    mix_w = swap_then_gather(mix_out, inner, outer, 0, 1)
    up_w = swap_then_gather(up_weight, inner, outer, 1, 0)
    down_w = swap_then_gather(down_weight, inner, outer, 0, 1)

    stream = tokens.astype(jnp.float32)
    normed = rms_scale(stream, mix_gain).astype(jnp.bfloat16)
    normed = lax.all_gather(normed, "fs", axis=0, axis_index_groups=inner, tiled=True)
    values = jnp.dot(normed, value_w, preferred_element_type=jnp.float32)
    gating = jnp.dot(normed, gate_w, preferred_element_type=jnp.float32)
    glu = (values * jax.nn.sigmoid(gating)).astype(jnp.bfloat16)
    channels = value_w.shape[1]
    taps = lax.dynamic_slice_in_dim(conv_taps, place * channels, channels, 1)
    gain = lax.dynamic_slice_in_dim(chan_gain, place * channels, channels, 0)
    convolved = depthwise(glu, taps)
    both = jnp.stack(
        (jnp.sum(convolved, axis=-1), jnp.sum(convolved * convolved, axis=-1))
    )
    both = jnp.sum(lax.all_gather(both, "fs", axis=0, axis_index_groups=inner), axis=0)
    both = lax.psum(both, "tp")
    centre = (both[0] / C)[:, None]
    spread = (both[1] / C)[:, None] - centre * centre
    hidden = jax.nn.silu((convolved - centre) * lax.rsqrt(spread + norm_floor) * gain).astype(
        jnp.bfloat16
    )
    mixed = shared_sum(
        jnp.dot(hidden, mix_w, preferred_element_type=jnp.float32).astype(jnp.bfloat16), inner, tp
    )
    own_rows = stream.shape[0] // tp
    own_stream = lax.dynamic_slice_in_dim(stream, lax.axis_index("tp") * own_rows, own_rows, 0)
    resid = own_stream + mixed
    normed_mlp = rms_scale(resid, mlp_gain).astype(jnp.bfloat16)
    normed_mlp = lax.all_gather(normed_mlp, "fs", axis=0, axis_index_groups=inner)
    normed_mlp = lax.all_gather(normed_mlp, "tp", axis=1).reshape(-1, normed.shape[1])
    active = jnp.square(
        jax.nn.relu(jnp.dot(normed_mlp, up_w, preferred_element_type=jnp.float32))
    ).astype(jnp.bfloat16)
    feed = shared_sum(
        jnp.dot(active, down_w, preferred_element_type=jnp.float32).astype(jnp.bfloat16), inner, tp
    )
    finished = (resid + feed).astype(jnp.bfloat16)
    return lax.all_gather(finished, "tp", axis=0, tiled=True)

MESH = pl.DeviceIdType.MESH
F32, BF16 = jnp.float32, jnp.bfloat16


def rows_at(start, size):
    return pl.ds(pl.multiple_of(start, 128), size)


def layer_kernel(
    ng,
    tok, mixg, gv, gg, taps, chg, mo, mlpg, up, dn,
    out,
    fgv, fgg, fmo, fup, fdn,
    tok_all, nrm, pad, cv, hid, st, st_all,
    acc, resid, nm_all, act, fin,
    sbo1, sbi1, rdo1, rdi1, sbo2, sbi2, rdo2, rdi2,
    ws, wr, lsem, tsem, nsem, ssem, rsem, fsem,
):
    f, t = lax.axis_index("fs"), lax.axis_index("tp")
    x, y = lax.rem(f, 2), lax.rem(lax.div(f, 2), 2)
    zp, zh = lax.rem(lax.div(f, 4), 2), lax.div(f, 8)
    sib = 1 - t
    L = tok.shape[0] // 2
    half = ng * L
    width = tok.shape[1]
    chans = fgv.shape[1]
    hidden = fup.shape[1]
    depth = gv.shape[0]
    sends = []

    def flip(coord, bit):
        return 1 - coord if bit else coord

    def chip(dq):
        return flip(zp, dq // 2) * 2 + flip(x, dq % 2)

    def fs_of(dq, do):
        return flip(zh, do // 2) * 8 + flip(zp, dq // 2) * 4 + flip(y, do % 2) * 2 + flip(x, dq % 2)

    p = chip(0)

    def push(src, dst, s_sem, r_sem, device):
        copy = pltpu.make_async_remote_copy(
            src_ref=src, dst_ref=dst, send_sem=s_sem, recv_sem=r_sem,
            device_id=device, device_id_type=MESH,
        )
        copy.start()
        sends.append(copy)

    def arrived(dst, s_sem, r_sem):
        pltpu.make_async_remote_copy(
            src_ref=dst, dst_ref=dst, send_sem=s_sem, recv_sem=r_sem,
            device_id=(f, sib), device_id_type=MESH,
        ).wait_recv()

    barrier = pltpu.get_barrier_semaphore()
    peers = [(fs_of(dq, 0), u) for dq in range(1, ng) for u in (t, sib)]
    peers += [(f, sib), (fs_of(0, 1), t), (fs_of(0, 2), t)]
    for peer in peers:
        pl.semaphore_signal(barrier, inc=1, device_id=peer, device_id_type=MESH)
    pl.semaphore_wait(barrier, len(peers))

    weights = (
        (lambda q: gv.at[:, rows_at(q * chans, chans)], lambda g: fgv.at[rows_at(g * depth, depth), :]),
        (lambda q: gg.at[:, rows_at(q * chans, chans)], lambda g: fgg.at[rows_at(g * depth, depth), :]),
        (lambda q: mo.at[rows_at(q * chans, chans), :], lambda g: fmo.at[:, rows_at(g * depth, depth)]),
        (lambda q: up.at[:, rows_at(q * hidden, hidden)], lambda g: fup.at[rows_at(g * depth, depth), :]),
        (lambda q: dn.at[rows_at(q * hidden, hidden), :], lambda g: fdn.at[:, rows_at(g * depth, depth)]),
    )

    def spread_in_plane(a):
        src, dst = weights[a]
        for dq in range(1, ng):
            push(src(chip(dq)), dst(f), ws.at[a, dq], wr.at[a, dq], (fs_of(dq, 0), t))

    def spread_own(a):
        src, dst = weights[a]
        for do in (2, 1):
            push(src(p), dst(f), ws.at[a, do * ng], wr.at[a, do * ng], (fs_of(0, do), t))

    def forward(a):
        dst = weights[a][1]
        for dq in range(1, ng):
            piece = dst(fs_of(dq, 0))
            arrived(piece, ws.at[a, 0], wr.at[a, dq])
            for do in (2, 1):
                push(piece, piece, ws.at[a, do * ng + dq], wr.at[a, do * ng + dq], (fs_of(0, do), t))

    def relay(a, which=(0, 1, 2, 3)):
        dst = weights[a][1]
        for dq in which:
            piece = dst(fs_of(dq, 2))
            arrived(piece, ws.at[a, 0], wr.at[a, 2 * ng + dq])
            push(piece, piece, ws.at[a, 3 * ng + dq], wr.at[a, 3 * ng + dq], (fs_of(0, 1), t))

    def whole(a):
        dst = weights[a][1]
        for do in (1, 3):
            for dq in range(ng):
                arrived(dst(fs_of(dq, do)), ws.at[a, 0], wr.at[a, do * ng + dq])
        local(a).wait()

    def local(a):
        src, dst = weights[a]
        return pltpu.make_async_copy(src(p), dst(f), lsem.at[a])

    for a in (0, 1):
        spread_in_plane(a)
    for a in (0, 1):
        spread_own(a)
    for dq in range(1, ng):
        push(
            tok.at[rows_at(t * L, L)], tok_all.at[rows_at(t * half + p * L, L)],
            tsem.at[0, dq], tsem.at[1, dq], (fs_of(dq, 0), t),
        )
    spread_in_plane(2)
    spread_own(2)
    for a in (3, 4):
        spread_in_plane(a)
    for a in range(5):
        local(a).start()

    step = 16

    def norm_rows(load, gain, dst, start):
        def body(i, _):
            value = load(i * step).astype(F32)
            scale = lax.rsqrt(jnp.mean(value * value, axis=-1, keepdims=True) + norm_floor)
            dst[pl.ds(pl.multiple_of(start + i * step, step), step), :] = (
                value * scale * gain[...]
            ).astype(BF16)
            return 0

        lax.fori_loop(0, L // step, body, 0)

    def from_ref(ref, base):
        return lambda i: ref[pl.ds(pl.multiple_of(base + i, step), step), :]

    for u in range(2):
        norm_rows(from_ref(tok, u * L), mixg, nrm, u * half + p * L)
    for a in (0, 1):
        forward(a)
    for dq in range(1, ng):
        block = tok_all.at[rows_at(t * half + chip(dq) * L, L)]
        arrived(block, tsem.at[0, 0], tsem.at[1, dq])
        push(block, block, tsem.at[2, dq], tsem.at[3, dq], (f, sib))
        norm_rows(from_ref(tok_all, t * half + chip(dq) * L), mixg, nrm, t * half + chip(dq) * L)
    forward(2)
    for a in (3, 4):
        spread_own(a)
    for dq in range(1, ng):
        start = sib * half + chip(dq) * L
        arrived(tok_all.at[rows_at(start, L)], tsem.at[0, 0], tsem.at[3, dq])
        norm_rows(from_ref(tok_all, start), mixg, nrm, start)

    relay(0)
    relay(1)
    whole(0)
    whole(1)
    pad[...] = jnp.zeros_like(pad)
    st[...] = jnp.zeros_like(st)
    taps_n = taps.shape[0]
    reach = taps_n // 2
    lead = (reach + 7) // 8 * 8
    own_cols = p * chans
    eye = lax.broadcasted_iota(jnp.int32, (L, L), 0) == lax.broadcasted_iota(jnp.int32, (L, L), 1)

    def conv_block(b, _):
        rows = rows_at(b * L, L)
        left = nrm[rows, :]
        values = jnp.dot(left, fgv[...], preferred_element_type=F32)
        gating = jnp.dot(left, fgg[...], preferred_element_type=F32)
        glu = (values * jax.nn.sigmoid(gating)).astype(BF16).astype(F32)
        pad[pl.ds(lead, L), :] = glu
        sums = jnp.zeros((L, 1), F32)
        squares = jnp.zeros((L, 1), F32)
        for c in range(chans // 128):
            total = jnp.zeros((L, 128), F32)
            for j in range(taps_n):
                tap = taps[pl.ds(j, 1), rows_at(own_cols + c * 128, 128)]
                total = total + pad[pl.ds(lead - reach + j, L), pl.ds(c * 128, 128)] * tap
            cv[rows, pl.ds(c * 128, 128)] = total
            sums = sums + jnp.sum(total, axis=1, keepdims=True)
            squares = squares + jnp.sum(total * total, axis=1, keepdims=True)
        st[b, pl.ds(0, 1), :] = jnp.sum(jnp.where(eye, sums, 0.0), axis=0, keepdims=True)
        st[b, pl.ds(1, 1), :] = jnp.sum(jnp.where(eye, squares, 0.0), axis=0, keepdims=True)
        return 0

    lax.fori_loop(0, 2 * ng, conv_block, 0)

    slots = [(dq, du) for dq in range(ng) for du in range(2) if (dq, du) != (0, 0)]
    for dq, du in slots:
        push(
            st, st_all.at[dq * 2 + du],
            ssem.at[0, dq * 2 + du], ssem.at[1, dq * 2 + du],
            (fs_of(dq, 0), t if du == 0 else sib),
        )
    forward(3)
    relay(2)
    for dq, du in slots:
        arrived(st_all.at[dq * 2 + du], ssem.at[0, 0], ssem.at[1, dq * 2 + du])

    def hidden_block(b, _):
        rows = rows_at(b * L, L)
        total = st[b]
        for dq, du in slots:
            total = total + st_all[dq * 2 + du, b]
        count = chans * ng * 2
        sums = jnp.sum(jnp.where(eye, total[0:1, :], 0.0), axis=1, keepdims=True)
        squares = jnp.sum(jnp.where(eye, total[1:2, :], 0.0), axis=1, keepdims=True)
        centre = sums / count
        spread = squares / count - centre * centre
        value = (cv[rows, :] - centre) * lax.rsqrt(spread + norm_floor)
        value = value * chg[:, rows_at(own_cols, chans)]
        hid[rows, :] = (value * jax.nn.sigmoid(value)).astype(BF16)
        return 0

    lax.fori_loop(0, 2 * ng, hidden_block, 0)

    cols = 512

    def reduce_rows(left, right, sbo, sbi, rdo, rdi, k):
        def theirs(n, _):
            at = rows_at(n * cols, cols)
            sbo[:, at] = jnp.dot(
                left[rows_at(sib * half, half), :], right[:, at], preferred_element_type=F32
            ).astype(BF16)
            return 0

        lax.fori_loop(0, width // cols, theirs, 0)
        push(sbo, sbi, rsem.at[k, 0], rsem.at[k, 1], (f, sib))

        def mine(n, _):
            at = rows_at(n * cols, cols)
            acc[:, at] = jnp.dot(
                left[rows_at(t * half, half), :], right[:, at], preferred_element_type=F32
            )
            return 0

        lax.fori_loop(0, width // cols, mine, 0)
        arrived(sbi, rsem.at[k, 0], rsem.at[k, 1])
        for dq in range(1, ng):
            base = chip(dq) * L

            def add(i, _):
                at = pl.ds(pl.multiple_of(base + i * step, step), step)
                rdo[at, :] = (acc[at, :] + sbi[at, :].astype(F32)).astype(BF16)
                return 0

            lax.fori_loop(0, L // step, add, 0)
            push(
                rdo.at[rows_at(base, L)], rdi.at[dq - 1],
                rsem.at[k, 2 * dq], rsem.at[k, 2 * dq + 1], (fs_of(dq, 0), t),
            )

    def reduced(sbi, rdi, i):
        at = pl.ds(pl.multiple_of(p * L + i * step, step), step)
        total = acc[at, :] + sbi[at, :].astype(F32)
        for dq in range(1, ng):
            total = total + rdi[dq - 1, pl.ds(pl.multiple_of(i * step, step), step), :].astype(F32)
        return total.astype(BF16).astype(F32)

    def wait_reduced(rdi, k):
        for dq in range(1, ng):
            arrived(rdi.at[dq - 1], rsem.at[k, 0], rsem.at[k, 2 * dq + 1])

    whole(2)
    reduce_rows(hid, fmo, sbo1, sbi1, rdo1, rdi1, 0)
    forward(4)
    wait_reduced(rdi1, 0)

    def resid_rows(i, _):
        at = pl.ds(pl.multiple_of(i * step, step), step)
        own = tok[pl.ds(pl.multiple_of(t * L + i * step, step), step), :].astype(F32)
        value = own + reduced(sbi1, rdi1, i)
        resid[at, :] = value
        scale = lax.rsqrt(jnp.mean(value * value, axis=-1, keepdims=True) + norm_floor)
        nm_all[pl.ds(pl.multiple_of(t * half + p * L + i * step, step), step), :] = (
            value * scale * mlpg[...]
        ).astype(BF16)
        return 0

    lax.fori_loop(0, L // step, resid_rows, 0)
    mine = nm_all.at[rows_at(t * half + p * L, L)]
    for dq in range(1, ng):
        push(mine, mine, nsem.at[0, dq], nsem.at[1, dq], (fs_of(dq, 0), t))
    push(mine, mine, nsem.at[2, 0], nsem.at[3, 0], (f, sib))
    relay(3)
    for dq in range(1, ng):
        block = nm_all.at[rows_at(t * half + chip(dq) * L, L)]
        arrived(block, nsem.at[0, 0], nsem.at[1, dq])
        push(block, block, nsem.at[2, dq], nsem.at[3, dq], (f, sib))

    whole(3)

    def up_half(u):
        def body(n, _):
            at = rows_at(n * 256, 256)
            value = jnp.dot(
                nm_all[rows_at(u * half, half), :], fup[:, at], preferred_element_type=F32
            )
            value = jnp.maximum(value, 0.0)
            act[rows_at(u * half, half), at] = (value * value).astype(BF16)
            return 0

        lax.fori_loop(0, hidden // 256, body, 0)

    up_half(t)
    relay(4, (0, 1))
    for dq in range(ng):
        arrived(nm_all.at[rows_at(sib * half + chip(dq) * L, L)], nsem.at[0, 0], nsem.at[3, dq])
    up_half(sib)
    relay(4, (2, 3))
    whole(4)
    reduce_rows(act, fdn, sbo2, sbi2, rdo2, rdi2, 1)
    wait_reduced(rdi2, 1)

    def finish_rows(i, _):
        at = pl.ds(pl.multiple_of(i * step, step), step)
        value = (resid[at, :] + reduced(sbi2, rdi2, i)).astype(BF16)
        fin[0, at, :] = value
        out[pl.ds(pl.multiple_of(t * L + i * step, step), step), :] = value
        return 0

    lax.fori_loop(0, L // step, finish_rows, 0)
    push(fin.at[0], fin.at[1], fsem.at[0], fsem.at[1], (f, sib))
    arrived(fin.at[1], fsem.at[0], fsem.at[1])

    def copy_rows(i, _):
        at = pl.ds(pl.multiple_of(i * step, step), step)
        out[pl.ds(pl.multiple_of(sib * L + i * step, step), step), :] = fin[1, at, :]
        return 0

    lax.fori_loop(0, L // step, copy_rows, 0)
    for copy in sends:
        copy.wait_send()


def fused_device(ng, nz, tokens, mix_gain, glu_value, glu_gate, conv_taps, chan_gain, mix_out, mlp_gain, up_weight, down_weight):
    rows, width = tokens.shape
    fs = ng * nz
    L = rows // 2
    half = ng * L
    chans = glu_value.shape[1] // ng
    hidden = up_weight.shape[1] // ng
    depth = glu_value.shape[0]
    blocks = 2 * ng
    vm = pltpu.VMEM
    dma = pltpu.SemaphoreType.DMA
    reduce_bufs = [
        vm((half, width), BF16), vm((half, width), BF16), vm((half, width), BF16),
        vm((ng - 1, L, width), BF16),
    ]
    scratch = [
        vm((fs * depth, chans), BF16), vm((fs * depth, chans), BF16), vm((chans, width), BF16),
        vm((fs * depth, hidden), BF16), vm((hidden, width), BF16),
        vm((2 * half, width), BF16), vm((2 * half, width), BF16),
        vm((L + 32, chans), F32), vm((2 * half, chans), F32), vm((2 * half, chans), BF16),
        vm((blocks, 8, L), F32), vm((blocks, blocks, 8, L), F32),
        vm((half, width), F32), vm((L, width), F32), vm((2 * half, width), BF16),
        vm((2 * half, hidden), BF16), vm((2, L, width), BF16),
        *reduce_bufs, *reduce_bufs,
        dma((5, fs)), dma((5, fs)), dma((5,)), dma((4, ng)), dma((4, ng)),
        dma((2, blocks)), dma((2, 2 * ng)), dma((2,)),
    ]
    return pl.pallas_call(
        functools.partial(layer_kernel, ng),
        out_shape=jax.ShapeDtypeStruct((rows, width), BF16),
        in_specs=[pl.BlockSpec(memory_space=vm)] * 10,
        out_specs=pl.BlockSpec(memory_space=vm),
        scratch_shapes=scratch,
        compiler_params=pltpu.CompilerParams(
            collective_id=0, has_side_effects=True, vmem_limit_bytes=60 * 1024 * 1024
        ),
    )(
        tokens, mix_gain[None], glu_value, glu_gate, conv_taps, chan_gain[None], mix_out,
        mlp_gain[None], up_weight, down_weight,
    )


def per_device(*args):
    tokens, glu_value, conv_taps = args[0], args[2], args[4]
    fs, tp = lax.axis_size("fs"), lax.axis_size("tp")
    group = 4
    fits = (
        tp == 2
        and fs == group * 4
        and tokens.shape[0] == 2 * LEN
        and glu_value.shape[0] % 128 == 0
        and conv_taps.shape[1] % (group * 128) == 0
        and conv_taps.shape[0] <= 31
    )
    if fits:
        return fused_device(group, fs // group, *args)
    return plain_device(*args)


def solution(mesh):
    in_specs = (
        P("fs", None),
        P(),
        P("fs", "tp"),
        P("fs", "tp"),
        P(None, "tp"),
        P("tp"),
        P("tp", "fs"),
        P(),
        P("fs", "tp"),
        P("tp", "fs"),
    )
    out_specs = P("fs", None)
    return jax.shard_map(
        per_device, mesh=mesh, in_specs=in_specs, out_specs=out_specs, check_vma=False
    )
```

```python
import functools

import jax
import jax.numpy as jnp
from jax import lax
from jax.experimental import pallas as pl
from jax.experimental.pallas import tpu as pltpu
from jax.sharding import PartitionSpec as P

C = 2048
LEN = 128


norm_floor = 0.05


def rms_scale(stream, gain):
    return stream * lax.rsqrt(jnp.mean(stream * stream, axis=-1, keepdims=True) + norm_floor) * gain


def bf16_round(value):
    return lax.optimization_barrier(value.astype(jnp.bfloat16)).astype(jnp.float32)


def depthwise(glu, conv_taps):
    seqs = glu.shape[0] // LEN
    blocks = glu.reshape(seqs, LEN, glu.shape[1]).astype(jnp.float32)
    reach = conv_taps.shape[0] // 2
    padded = jnp.pad(blocks, ((0, 0), (reach, reach), (0, 0)))
    total = jnp.zeros_like(blocks)
    for offset in range(conv_taps.shape[0]):
        total = total + padded[:, offset : offset + LEN] * conv_taps[offset]
    return total.reshape(glu.shape)


def swap_then_gather(weight, inner, outer, split, join):
    own = lax.all_to_all(
        weight, "fs", split_axis=split, concat_axis=join, axis_index_groups=inner, tiled=True
    )
    return lax.all_gather(own, "fs", axis=join, axis_index_groups=outer, tiled=True)


def shared_sum(partial, inner, tp):
    part = lax.all_to_all(
        partial, "fs", split_axis=0, concat_axis=0, axis_index_groups=inner, tiled=True
    )
    group = len(inner[0])
    rows = partial.shape[0] // group
    part = part.reshape(group, tp, rows // tp, -1).transpose(1, 0, 2, 3)
    part = lax.all_to_all(part, "tp", split_axis=0, concat_axis=0, tiled=True)
    return bf16_round(jnp.sum(part.astype(jnp.float32), axis=(0, 1)))


def plain_device(
    tokens,
    mix_gain,
    glu_value,
    glu_gate,
    conv_taps,
    chan_gain,
    mix_out,
    mlp_gain,
    up_weight,
    down_weight,
):
    fs, tp = lax.axis_size("fs"), lax.axis_size("tp")
    group = 4 if fs % 4 == 0 else 1
    inner = [[o * group + i for i in range(group)] for o in range(fs // group)]
    outer = [[o * group + i for o in range(fs // group)] for i in range(group)]
    place = lax.rem(lax.axis_index("fs"), group)

    value_w = swap_then_gather(glu_value, inner, outer, 1, 0)
    gate_w = swap_then_gather(glu_gate, inner, outer, 1, 0)
    mix_w = swap_then_gather(mix_out, inner, outer, 0, 1)
    up_w = swap_then_gather(up_weight, inner, outer, 1, 0)
    down_w = swap_then_gather(down_weight, inner, outer, 0, 1)

    stream = tokens.astype(jnp.float32)
    normed = rms_scale(stream, mix_gain).astype(jnp.bfloat16)
    normed = lax.all_gather(normed, "fs", axis=0, axis_index_groups=inner, tiled=True)
    values = jnp.dot(normed, value_w, preferred_element_type=jnp.float32)
    gating = jnp.dot(normed, gate_w, preferred_element_type=jnp.float32)
    glu = (values * jax.nn.sigmoid(gating)).astype(jnp.bfloat16)
    channels = value_w.shape[1]
    taps = lax.dynamic_slice_in_dim(conv_taps, place * channels, channels, 1)
    gain = lax.dynamic_slice_in_dim(chan_gain, place * channels, channels, 0)
    convolved = depthwise(glu, taps)
    both = jnp.stack(
        (jnp.sum(convolved, axis=-1), jnp.sum(convolved * convolved, axis=-1))
    )
    both = jnp.sum(lax.all_gather(both, "fs", axis=0, axis_index_groups=inner), axis=0)
    both = lax.psum(both, "tp")
    centre = (both[0] / C)[:, None]
    spread = (both[1] / C)[:, None] - centre * centre
    hidden = jax.nn.silu((convolved - centre) * lax.rsqrt(spread + norm_floor) * gain).astype(
        jnp.bfloat16
    )
    mixed = shared_sum(
        jnp.dot(hidden, mix_w, preferred_element_type=jnp.float32).astype(jnp.bfloat16), inner, tp
    )
    own_rows = stream.shape[0] // tp
    own_stream = lax.dynamic_slice_in_dim(stream, lax.axis_index("tp") * own_rows, own_rows, 0)
    resid = own_stream + mixed
    normed_mlp = rms_scale(resid, mlp_gain).astype(jnp.bfloat16)
    normed_mlp = lax.all_gather(normed_mlp, "fs", axis=0, axis_index_groups=inner)
    normed_mlp = lax.all_gather(normed_mlp, "tp", axis=1).reshape(-1, normed.shape[1])
    active = jnp.square(
        jax.nn.relu(jnp.dot(normed_mlp, up_w, preferred_element_type=jnp.float32))
    ).astype(jnp.bfloat16)
    feed = shared_sum(
        jnp.dot(active, down_w, preferred_element_type=jnp.float32).astype(jnp.bfloat16), inner, tp
    )
    finished = (resid + feed).astype(jnp.bfloat16)
    return lax.all_gather(finished, "tp", axis=0, tiled=True)

MESH = pl.DeviceIdType.MESH
F32, BF16 = jnp.float32, jnp.bfloat16


def rows_at(start, size):
    return pl.ds(pl.multiple_of(start, 128), size)


def layer_kernel(
    ng,
    tok, mixg, gv, gg, taps, chg, mo, mlpg, up, dn,
    out,
    fgv, fgg, fmo, fup, fdn,
    tok_all, nrm, pad, cv, hid, st, st_all,
    acc, resid, nm_all, act, fin,
    sbo1, sbi1, rdo1, rdi1, sbo2, sbi2, rdo2, rdi2,
    ws, wr, lsem, tsem, nsem, ssem, rsem, fsem,
):
    f, t = lax.axis_index("fs"), lax.axis_index("tp")
    x, y = lax.rem(f, 2), lax.rem(lax.div(f, 2), 2)
    zp, zh = lax.rem(lax.div(f, 4), 2), lax.div(f, 8)
    sib = 1 - t
    L = tok.shape[0] // 2
    half = ng * L
    width = tok.shape[1]
    chans = fgv.shape[1]
    hidden = fup.shape[1]
    depth = gv.shape[0]
    sends = []

    def flip(coord, bit):
        return 1 - coord if bit else coord

    def chip(dq):
        return flip(zp, dq // 2) * 2 + flip(x, dq % 2)

    def fs_of(dq, do):
        return flip(zh, do // 2) * 8 + flip(zp, dq // 2) * 4 + flip(y, do % 2) * 2 + flip(x, dq % 2)

    p = chip(0)

    def push(src, dst, s_sem, r_sem, device):
        copy = pltpu.make_async_remote_copy(
            src_ref=src, dst_ref=dst, send_sem=s_sem, recv_sem=r_sem,
            device_id=device, device_id_type=MESH,
        )
        copy.start()
        sends.append(copy)

    def arrived(dst, s_sem, r_sem):
        pltpu.make_async_remote_copy(
            src_ref=dst, dst_ref=dst, send_sem=s_sem, recv_sem=r_sem,
            device_id=(f, sib), device_id_type=MESH,
        ).wait_recv()

    barrier = pltpu.get_barrier_semaphore()
    peers = [(fs_of(dq, 0), u) for dq in range(1, ng) for u in (t, sib)]
    peers += [(f, sib), (fs_of(0, 1), t), (fs_of(0, 2), t)]
    for peer in peers:
        pl.semaphore_signal(barrier, inc=1, device_id=peer, device_id_type=MESH)
    pl.semaphore_wait(barrier, len(peers))

    weights = (
        (lambda q: gv.at[:, rows_at(q * chans, chans)], lambda g: fgv.at[rows_at(g * depth, depth), :]),
        (lambda q: gg.at[:, rows_at(q * chans, chans)], lambda g: fgg.at[rows_at(g * depth, depth), :]),
        (lambda q: mo.at[rows_at(q * chans, chans), :], lambda g: fmo.at[:, rows_at(g * depth, depth)]),
        (lambda q: up.at[:, rows_at(q * hidden, hidden)], lambda g: fup.at[rows_at(g * depth, depth), :]),
        (lambda q: dn.at[rows_at(q * hidden, hidden), :], lambda g: fdn.at[:, rows_at(g * depth, depth)]),
    )

    def spread_in_plane(a):
        src, dst = weights[a]
        for dq in range(1, ng):
            push(src(chip(dq)), dst(f), ws.at[a, dq], wr.at[a, dq], (fs_of(dq, 0), t))

    def spread_own(a):
        src, dst = weights[a]
        for do in (2, 1):
            push(src(p), dst(f), ws.at[a, do * ng], wr.at[a, do * ng], (fs_of(0, do), t))

    def forward(a):
        dst = weights[a][1]
        for dq in range(1, ng):
            piece = dst(fs_of(dq, 0))
            arrived(piece, ws.at[a, 0], wr.at[a, dq])
            for do in (2, 1):
                push(piece, piece, ws.at[a, do * ng + dq], wr.at[a, do * ng + dq], (fs_of(0, do), t))

    def relay(a, which=(0, 1, 2, 3)):
        dst = weights[a][1]
        for dq in which:
            piece = dst(fs_of(dq, 2))
            arrived(piece, ws.at[a, 0], wr.at[a, 2 * ng + dq])
            push(piece, piece, ws.at[a, 3 * ng + dq], wr.at[a, 3 * ng + dq], (fs_of(0, 1), t))

    def whole(a):
        dst = weights[a][1]
        for do in (1, 3):
            for dq in range(ng):
                arrived(dst(fs_of(dq, do)), ws.at[a, 0], wr.at[a, do * ng + dq])
        local(a).wait()

    def local(a):
        src, dst = weights[a]
        return pltpu.make_async_copy(src(p), dst(f), lsem.at[a])

    for a in (0, 1):
        spread_in_plane(a)
    for dq in (2, 1):
        push(
            tok.at[rows_at(t * L, L)], tok_all.at[rows_at(t * half + p * L, L)],
            tsem.at[0, dq], tsem.at[1, dq], (fs_of(dq, 0), t),
        )
    spread_in_plane(2)
    for a in (0, 1, 2):
        spread_own(a)
    for a in (3, 4):
        spread_in_plane(a)
    for a in range(5):
        local(a).start()

    step = 16

    def norm_rows(load, gain, dst, start):
        def body(i, _):
            value = load(i * step).astype(F32)
            scale = lax.rsqrt(jnp.mean(value * value, axis=-1, keepdims=True) + norm_floor)
            dst[pl.ds(pl.multiple_of(start + i * step, step), step), :] = (
                value * scale * gain[...]
            ).astype(BF16)
            return 0

        lax.fori_loop(0, L // step, body, 0)

    def from_ref(ref, base):
        return lambda i: ref[pl.ds(pl.multiple_of(base + i, step), step), :]

    for u in range(2):
        norm_rows(from_ref(tok, u * L), mixg, nrm, u * half + p * L)
    for a in (0, 1):
        forward(a)
    for dq in (2, 1, 3):
        block = tok_all.at[rows_at(t * half + chip(dq) * L, L)]
        arrived(block, tsem.at[0, 0], tsem.at[1, dq])
        if dq == 2:
            push(block, block, tsem.at[0, 3], tsem.at[1, 3], (fs_of(1, 0), t))
        push(block, block, tsem.at[2, dq], tsem.at[3, dq], (f, sib))
        norm_rows(from_ref(tok_all, t * half + chip(dq) * L), mixg, nrm, t * half + chip(dq) * L)
    forward(2)
    for a in (3, 4):
        spread_own(a)
    for dq in range(1, ng):
        start = sib * half + chip(dq) * L
        arrived(tok_all.at[rows_at(start, L)], tsem.at[0, 0], tsem.at[3, dq])
        norm_rows(from_ref(tok_all, start), mixg, nrm, start)

    relay(0)
    relay(1)
    whole(0)
    whole(1)
    pad[...] = jnp.zeros_like(pad)
    st[...] = jnp.zeros_like(st)
    taps_n = taps.shape[0]
    reach = taps_n // 2
    lead = (reach + 7) // 8 * 8
    own_cols = p * chans
    eye = lax.broadcasted_iota(jnp.int32, (L, L), 0) == lax.broadcasted_iota(jnp.int32, (L, L), 1)

    def conv_block(b, _):
        rows = rows_at(b * L, L)
        left = nrm[rows, :]
        values = jnp.dot(left, fgv[...], preferred_element_type=F32)
        gating = jnp.dot(left, fgg[...], preferred_element_type=F32)
        glu = (values * jax.nn.sigmoid(gating)).astype(BF16).astype(F32)
        pad[pl.ds(lead, L), :] = glu
        sums = jnp.zeros((L, 1), F32)
        squares = jnp.zeros((L, 1), F32)
        for c in range(chans // 128):
            total = jnp.zeros((L, 128), F32)
            for j in range(taps_n):
                tap = taps[pl.ds(j, 1), rows_at(own_cols + c * 128, 128)]
                total = total + pad[pl.ds(lead - reach + j, L), pl.ds(c * 128, 128)] * tap
            cv[rows, pl.ds(c * 128, 128)] = total
            sums = sums + jnp.sum(total, axis=1, keepdims=True)
            squares = squares + jnp.sum(total * total, axis=1, keepdims=True)
        st[b, pl.ds(0, 1), :] = jnp.sum(jnp.where(eye, sums, 0.0), axis=0, keepdims=True)
        st[b, pl.ds(1, 1), :] = jnp.sum(jnp.where(eye, squares, 0.0), axis=0, keepdims=True)
        return 0

    lax.fori_loop(0, 2 * ng, conv_block, 0)

    slots = [(dq, du) for dq in range(ng) for du in range(2) if (dq, du) != (0, 0)]
    for dq, du in slots:
        push(
            st, st_all.at[dq * 2 + du],
            ssem.at[0, dq * 2 + du], ssem.at[1, dq * 2 + du],
            (fs_of(dq, 0), t if du == 0 else sib),
        )
    forward(3)
    relay(2)
    for dq, du in slots:
        arrived(st_all.at[dq * 2 + du], ssem.at[0, 0], ssem.at[1, dq * 2 + du])

    def hidden_block(b, _):
        rows = rows_at(b * L, L)
        total = st[b]
        for dq, du in slots:
            total = total + st_all[dq * 2 + du, b]
        count = chans * ng * 2
        sums = jnp.sum(jnp.where(eye, total[0:1, :], 0.0), axis=1, keepdims=True)
        squares = jnp.sum(jnp.where(eye, total[1:2, :], 0.0), axis=1, keepdims=True)
        centre = sums / count
        spread = squares / count - centre * centre
        value = (cv[rows, :] - centre) * lax.rsqrt(spread + norm_floor)
        value = value * chg[:, rows_at(own_cols, chans)]
        hid[rows, :] = (value * jax.nn.sigmoid(value)).astype(BF16)
        return 0

    lax.fori_loop(0, 2 * ng, hidden_block, 0)

    cols = 512

    def reduce_rows(left, right, sbo, sbi, rdo, rdi, k):
        def theirs(n, _):
            at = rows_at(n * cols, cols)
            sbo[:, at] = jnp.dot(
                left[rows_at(sib * half, half), :], right[:, at], preferred_element_type=F32
            ).astype(BF16)
            return 0

        lax.fori_loop(0, width // cols, theirs, 0)
        push(sbo, sbi, rsem.at[k, 0], rsem.at[k, 1], (f, sib))

        def mine(n, _):
            at = rows_at(n * cols, cols)
            acc[:, at] = jnp.dot(
                left[rows_at(t * half, half), :], right[:, at], preferred_element_type=F32
            )
            return 0

        lax.fori_loop(0, width // cols, mine, 0)
        arrived(sbi, rsem.at[k, 0], rsem.at[k, 1])
        for dq in (3, 1, 2):
            base = chip(dq) * L
            if dq == 2:
                arrived(rdi.at[2], rsem.at[k, 0], rsem.at[k, 7])

            def add(i, _):
                at = pl.ds(pl.multiple_of(base + i * step, step), step)
                value = acc[at, :] + sbi[at, :].astype(F32)
                if dq == 2:
                    value = value + rdi[2, pl.ds(pl.multiple_of(i * step, step), step), :].astype(F32)
                rdo[at, :] = value.astype(BF16)
                return 0

            lax.fori_loop(0, L // step, add, 0)
            push(
                rdo.at[rows_at(base, L)], rdi.at[dq - 1],
                rsem.at[k, 2 * dq], rsem.at[k, 2 * dq + 1],
                (fs_of(2 if dq == 2 else 1, 0), t),
            )

    def reduced(sbi, rdi, i):
        at = pl.ds(pl.multiple_of(p * L + i * step, step), step)
        total = acc[at, :] + sbi[at, :].astype(F32)
        for dq in (1, 2):
            total = total + rdi[dq - 1, pl.ds(pl.multiple_of(i * step, step), step), :].astype(F32)
        return total.astype(BF16).astype(F32)

    def wait_reduced(rdi, k):
        for dq in (1, 2):
            arrived(rdi.at[dq - 1], rsem.at[k, 0], rsem.at[k, 2 * dq + 1])

    whole(2)
    reduce_rows(hid, fmo, sbo1, sbi1, rdo1, rdi1, 0)
    forward(4)
    wait_reduced(rdi1, 0)

    def resid_rows(i, _):
        at = pl.ds(pl.multiple_of(i * step, step), step)
        own = tok[pl.ds(pl.multiple_of(t * L + i * step, step), step), :].astype(F32)
        value = own + reduced(sbi1, rdi1, i)
        resid[at, :] = value
        scale = lax.rsqrt(jnp.mean(value * value, axis=-1, keepdims=True) + norm_floor)
        nm_all[pl.ds(pl.multiple_of(t * half + p * L + i * step, step), step), :] = (
            value * scale * mlpg[...]
        ).astype(BF16)
        return 0

    lax.fori_loop(0, L // step, resid_rows, 0)
    mine = nm_all.at[rows_at(t * half + p * L, L)]
    for dq in (2, 1):
        push(mine, mine, nsem.at[0, dq], nsem.at[1, dq], (fs_of(dq, 0), t))
    push(mine, mine, nsem.at[2, 0], nsem.at[3, 0], (f, sib))
    for dq in (2, 1, 3):
        block = nm_all.at[rows_at(t * half + chip(dq) * L, L)]
        if dq == 3:
            relay(3)
        arrived(block, nsem.at[0, 0], nsem.at[1, dq])
        if dq == 2:
            push(block, block, nsem.at[0, 3], nsem.at[1, 3], (fs_of(1, 0), t))
        push(block, block, nsem.at[2, dq], nsem.at[3, dq], (f, sib))

    whole(3)

    def up_half(u):
        def body(n, _):
            at = rows_at(n * 256, 256)
            value = jnp.dot(
                nm_all[rows_at(u * half, half), :], fup[:, at], preferred_element_type=F32
            )
            value = jnp.maximum(value, 0.0)
            act[rows_at(u * half, half), at] = (value * value).astype(BF16)
            return 0

        lax.fori_loop(0, hidden // 256, body, 0)

    up_half(t)
    relay(4, (0, 1))
    for dq in range(ng):
        arrived(nm_all.at[rows_at(sib * half + chip(dq) * L, L)], nsem.at[0, 0], nsem.at[3, dq])
    up_half(sib)
    relay(4, (2, 3))
    whole(4)
    reduce_rows(act, fdn, sbo2, sbi2, rdo2, rdi2, 1)
    wait_reduced(rdi2, 1)

    def finish_rows(i, _):
        at = pl.ds(pl.multiple_of(i * step, step), step)
        value = (resid[at, :] + reduced(sbi2, rdi2, i)).astype(BF16)
        fin[0, at, :] = value
        out[pl.ds(pl.multiple_of(t * L + i * step, step), step), :] = value
        return 0

    lax.fori_loop(0, L // step, finish_rows, 0)
    push(fin.at[0], fin.at[1], fsem.at[0], fsem.at[1], (f, sib))
    arrived(fin.at[1], fsem.at[0], fsem.at[1])

    def copy_rows(i, _):
        at = pl.ds(pl.multiple_of(i * step, step), step)
        out[pl.ds(pl.multiple_of(sib * L + i * step, step), step), :] = fin[1, at, :]
        return 0

    lax.fori_loop(0, L // step, copy_rows, 0)
    for copy in sends:
        copy.wait_send()


def fused_device(ng, nz, tokens, mix_gain, glu_value, glu_gate, conv_taps, chan_gain, mix_out, mlp_gain, up_weight, down_weight):
    rows, width = tokens.shape
    fs = ng * nz
    L = rows // 2
    half = ng * L
    chans = glu_value.shape[1] // ng
    hidden = up_weight.shape[1] // ng
    depth = glu_value.shape[0]
    blocks = 2 * ng
    vm = pltpu.VMEM
    dma = pltpu.SemaphoreType.DMA
    reduce_bufs = [
        vm((half, width), BF16), vm((half, width), BF16), vm((half, width), BF16),
        vm((ng - 1, L, width), BF16),
    ]
    scratch = [
        vm((fs * depth, chans), BF16), vm((fs * depth, chans), BF16), vm((chans, width), BF16),
        vm((fs * depth, hidden), BF16), vm((hidden, width), BF16),
        vm((2 * half, width), BF16), vm((2 * half, width), BF16),
        vm((L + 32, chans), F32), vm((2 * half, chans), F32), vm((2 * half, chans), BF16),
        vm((blocks, 8, L), F32), vm((blocks, blocks, 8, L), F32),
        vm((half, width), F32), vm((L, width), F32), vm((2 * half, width), BF16),
        vm((2 * half, hidden), BF16), vm((2, L, width), BF16),
        *reduce_bufs, *reduce_bufs,
        dma((5, fs)), dma((5, fs)), dma((5,)), dma((4, ng)), dma((4, ng)),
        dma((2, blocks)), dma((2, 2 * ng)), dma((2,)),
    ]
    return pl.pallas_call(
        functools.partial(layer_kernel, ng),
        out_shape=jax.ShapeDtypeStruct((rows, width), BF16),
        in_specs=[pl.BlockSpec(memory_space=vm)] * 10,
        out_specs=pl.BlockSpec(memory_space=vm),
        scratch_shapes=scratch,
        compiler_params=pltpu.CompilerParams(
            collective_id=0, has_side_effects=True, vmem_limit_bytes=60 * 1024 * 1024
        ),
    )(
        tokens, mix_gain[None], glu_value, glu_gate, conv_taps, chan_gain[None], mix_out,
        mlp_gain[None], up_weight, down_weight,
    )


def per_device(*args):
    tokens, glu_value, conv_taps = args[0], args[2], args[4]
    fs, tp = lax.axis_size("fs"), lax.axis_size("tp")
    group = 4
    fits = (
        tp == 2
        and fs == group * 4
        and tokens.shape[0] == 2 * LEN
        and glu_value.shape[0] % 128 == 0
        and conv_taps.shape[1] % (group * 128) == 0
        and conv_taps.shape[0] <= 31
    )
    if fits:
        return fused_device(group, fs // group, *args)
    return plain_device(*args)


def solution(mesh):
    in_specs = (
        P("fs", None),
        P(),
        P("fs", "tp"),
        P("fs", "tp"),
        P(None, "tp"),
        P("tp"),
        P("tp", "fs"),
        P(),
        P("fs", "tp"),
        P("tp", "fs"),
    )
    out_specs = P("fs", None)
    return jax.shard_map(
        per_device, mesh=mesh, in_specs=in_specs, out_specs=out_specs, check_vma=False
    )
```

```python
import functools

import jax
import jax.numpy as jnp
from jax import lax
from jax.experimental import pallas as pl
from jax.experimental.pallas import tpu as pltpu
from jax.sharding import PartitionSpec as P

C = 2048
LEN = 128


norm_floor = 0.05


def rms_scale(stream, gain):
    return stream * lax.rsqrt(jnp.mean(stream * stream, axis=-1, keepdims=True) + norm_floor) * gain


def bf16_round(value):
    return lax.optimization_barrier(value.astype(jnp.bfloat16)).astype(jnp.float32)


def depthwise(glu, conv_taps):
    seqs = glu.shape[0] // LEN
    blocks = glu.reshape(seqs, LEN, glu.shape[1]).astype(jnp.float32)
    reach = conv_taps.shape[0] // 2
    padded = jnp.pad(blocks, ((0, 0), (reach, reach), (0, 0)))
    total = jnp.zeros_like(blocks)
    for offset in range(conv_taps.shape[0]):
        total = total + padded[:, offset : offset + LEN] * conv_taps[offset]
    return total.reshape(glu.shape)


def swap_then_gather(weight, inner, outer, split, join):
    own = lax.all_to_all(
        weight, "fs", split_axis=split, concat_axis=join, axis_index_groups=inner, tiled=True
    )
    return lax.all_gather(own, "fs", axis=join, axis_index_groups=outer, tiled=True)


def shared_sum(partial, inner, tp):
    part = lax.all_to_all(
        partial, "fs", split_axis=0, concat_axis=0, axis_index_groups=inner, tiled=True
    )
    group = len(inner[0])
    rows = partial.shape[0] // group
    part = part.reshape(group, tp, rows // tp, -1).transpose(1, 0, 2, 3)
    part = lax.all_to_all(part, "tp", split_axis=0, concat_axis=0, tiled=True)
    return bf16_round(jnp.sum(part.astype(jnp.float32), axis=(0, 1)))


def plain_device(
    tokens,
    mix_gain,
    glu_value,
    glu_gate,
    conv_taps,
    chan_gain,
    mix_out,
    mlp_gain,
    up_weight,
    down_weight,
):
    fs, tp = lax.axis_size("fs"), lax.axis_size("tp")
    group = 4 if fs % 4 == 0 else 1
    inner = [[o * group + i for i in range(group)] for o in range(fs // group)]
    outer = [[o * group + i for o in range(fs // group)] for i in range(group)]
    place = lax.rem(lax.axis_index("fs"), group)

    value_w = swap_then_gather(glu_value, inner, outer, 1, 0)
    gate_w = swap_then_gather(glu_gate, inner, outer, 1, 0)
    mix_w = swap_then_gather(mix_out, inner, outer, 0, 1)
    up_w = swap_then_gather(up_weight, inner, outer, 1, 0)
    down_w = swap_then_gather(down_weight, inner, outer, 0, 1)

    stream = tokens.astype(jnp.float32)
    normed = rms_scale(stream, mix_gain).astype(jnp.bfloat16)
    normed = lax.all_gather(normed, "fs", axis=0, axis_index_groups=inner, tiled=True)
    values = jnp.dot(normed, value_w, preferred_element_type=jnp.float32)
    gating = jnp.dot(normed, gate_w, preferred_element_type=jnp.float32)
    glu = (values * jax.nn.sigmoid(gating)).astype(jnp.bfloat16)
    channels = value_w.shape[1]
    taps = lax.dynamic_slice_in_dim(conv_taps, place * channels, channels, 1)
    gain = lax.dynamic_slice_in_dim(chan_gain, place * channels, channels, 0)
    convolved = depthwise(glu, taps)
    both = jnp.stack(
        (jnp.sum(convolved, axis=-1), jnp.sum(convolved * convolved, axis=-1))
    )
    both = jnp.sum(lax.all_gather(both, "fs", axis=0, axis_index_groups=inner), axis=0)
    both = lax.psum(both, "tp")
    centre = (both[0] / C)[:, None]
    spread = (both[1] / C)[:, None] - centre * centre
    hidden = jax.nn.silu((convolved - centre) * lax.rsqrt(spread + norm_floor) * gain).astype(
        jnp.bfloat16
    )
    mixed = shared_sum(
        jnp.dot(hidden, mix_w, preferred_element_type=jnp.float32).astype(jnp.bfloat16), inner, tp
    )
    own_rows = stream.shape[0] // tp
    own_stream = lax.dynamic_slice_in_dim(stream, lax.axis_index("tp") * own_rows, own_rows, 0)
    resid = own_stream + mixed
    normed_mlp = rms_scale(resid, mlp_gain).astype(jnp.bfloat16)
    normed_mlp = lax.all_gather(normed_mlp, "fs", axis=0, axis_index_groups=inner)
    normed_mlp = lax.all_gather(normed_mlp, "tp", axis=1).reshape(-1, normed.shape[1])
    active = jnp.square(
        jax.nn.relu(jnp.dot(normed_mlp, up_w, preferred_element_type=jnp.float32))
    ).astype(jnp.bfloat16)
    feed = shared_sum(
        jnp.dot(active, down_w, preferred_element_type=jnp.float32).astype(jnp.bfloat16), inner, tp
    )
    finished = (resid + feed).astype(jnp.bfloat16)
    return lax.all_gather(finished, "tp", axis=0, tiled=True)

MESH = pl.DeviceIdType.MESH
F32, BF16 = jnp.float32, jnp.bfloat16


def rows_at(start, size):
    return pl.ds(pl.multiple_of(start, 128), size)


def layer_kernel(
    ng,
    tok, mixg, gv, gg, taps, chg, mo, mlpg, up, dn,
    out,
    fgv, fgg, fmo, fup, fdn,
    tok_all, nrm, pad, cv, hid, st, st_all,
    acc, resid, nm_all, act, fin,
    sbo1, sbi1, rdo1, rdi1, sbo2, sbi2, rdo2, rdi2,
    ws, wr, lsem, tsem, nsem, ssem, rsem, fsem,
):
    f, t = lax.axis_index("fs"), lax.axis_index("tp")
    x, y = lax.rem(f, 2), lax.rem(lax.div(f, 2), 2)
    zp, zh = lax.rem(lax.div(f, 4), 2), lax.div(f, 8)
    sib = 1 - t
    L = tok.shape[0] // 2
    half = ng * L
    width = tok.shape[1]
    chans = fgv.shape[1]
    hidden = fup.shape[1]
    depth = gv.shape[0]
    sends = []

    def flip(coord, bit):
        return 1 - coord if bit else coord

    def chip(dq):
        return flip(zp, dq // 2) * 2 + flip(x, dq % 2)

    def fs_of(dq, do):
        return flip(zh, do // 2) * 8 + flip(zp, dq // 2) * 4 + flip(y, do % 2) * 2 + flip(x, dq % 2)

    p = chip(0)

    def push(src, dst, s_sem, r_sem, device):
        copy = pltpu.make_async_remote_copy(
            src_ref=src, dst_ref=dst, send_sem=s_sem, recv_sem=r_sem,
            device_id=device, device_id_type=MESH,
        )
        copy.start()
        sends.append(copy)

    def arrived(dst, s_sem, r_sem):
        pltpu.make_async_remote_copy(
            src_ref=dst, dst_ref=dst, send_sem=s_sem, recv_sem=r_sem,
            device_id=(f, sib), device_id_type=MESH,
        ).wait_recv()

    barrier = pltpu.get_barrier_semaphore()
    peers = [(fs_of(dq, 0), u) for dq in range(1, ng) for u in (t, sib)]
    peers += [(f, sib), (fs_of(0, 1), t), (fs_of(0, 2), t)]
    for peer in peers:
        pl.semaphore_signal(barrier, inc=1, device_id=peer, device_id_type=MESH)
    pl.semaphore_wait(barrier, len(peers))

    weights = (
        (lambda q: gv.at[:, rows_at(q * chans, chans)], lambda g: fgv.at[rows_at(g * depth, depth), :]),
        (lambda q: gg.at[:, rows_at(q * chans, chans)], lambda g: fgg.at[rows_at(g * depth, depth), :]),
        (lambda q: mo.at[rows_at(q * chans, chans), :], lambda g: fmo.at[:, rows_at(g * depth, depth)]),
        (lambda q: up.at[:, rows_at(q * hidden, hidden)], lambda g: fup.at[rows_at(g * depth, depth), :]),
        (lambda q: dn.at[rows_at(q * hidden, hidden), :], lambda g: fdn.at[:, rows_at(g * depth, depth)]),
    )

    def spread_in_plane(a):
        src, dst = weights[a]
        for dq in range(1, ng):
            push(src(chip(dq)), dst(f), ws.at[a, dq], wr.at[a, dq], (fs_of(dq, 0), t))

    def spread_own(a):
        src, dst = weights[a]
        for do in (2, 1):
            push(src(p), dst(f), ws.at[a, do * ng], wr.at[a, do * ng], (fs_of(0, do), t))

    def forward(a):
        dst = weights[a][1]
        for dq in range(1, ng):
            piece = dst(fs_of(dq, 0))
            arrived(piece, ws.at[a, 0], wr.at[a, dq])
            for do in (2, 1):
                push(piece, piece, ws.at[a, do * ng + dq], wr.at[a, do * ng + dq], (fs_of(0, do), t))

    def relay(a, which=(0, 1, 2, 3)):
        dst = weights[a][1]
        for dq in which:
            piece = dst(fs_of(dq, 2))
            arrived(piece, ws.at[a, 0], wr.at[a, 2 * ng + dq])
            push(piece, piece, ws.at[a, 3 * ng + dq], wr.at[a, 3 * ng + dq], (fs_of(0, 1), t))

    def whole(a):
        dst = weights[a][1]
        for do in (1, 3):
            for dq in range(ng):
                arrived(dst(fs_of(dq, do)), ws.at[a, 0], wr.at[a, do * ng + dq])
        local(a).wait()

    def local(a):
        src, dst = weights[a]
        return pltpu.make_async_copy(src(p), dst(f), lsem.at[a])

    for a in (0, 1):
        spread_in_plane(a)
    for a in (0, 1):
        spread_own(a)
    for dq in range(1, ng):
        push(
            tok.at[rows_at(t * L, L)], tok_all.at[rows_at(t * half + p * L, L)],
            tsem.at[0, dq], tsem.at[1, dq], (fs_of(dq, 0), t),
        )
    spread_in_plane(2)
    spread_own(2)
    for a in (3, 4):
        spread_in_plane(a)
    for a in range(5):
        local(a).start()

    step = 16

    def norm_rows(load, gain, dst, start):
        def body(i, _):
            value = load(i * step).astype(F32)
            scale = lax.rsqrt(jnp.mean(value * value, axis=-1, keepdims=True) + norm_floor)
            dst[pl.ds(pl.multiple_of(start + i * step, step), step), :] = (
                value * scale * gain[...]
            ).astype(BF16)
            return 0

        lax.fori_loop(0, L // step, body, 0)

    def from_ref(ref, base):
        return lambda i: ref[pl.ds(pl.multiple_of(base + i, step), step), :]

    for u in range(2):
        norm_rows(from_ref(tok, u * L), mixg, nrm, u * half + p * L)
    for a in (0, 1):
        forward(a)
    for dq in range(1, ng):
        block = tok_all.at[rows_at(t * half + chip(dq) * L, L)]
        arrived(block, tsem.at[0, 0], tsem.at[1, dq])
        push(block, block, tsem.at[2, dq], tsem.at[3, dq], (f, sib))
        norm_rows(from_ref(tok_all, t * half + chip(dq) * L), mixg, nrm, t * half + chip(dq) * L)
    forward(2)
    for a in (3, 4):
        spread_own(a)
    for dq in range(1, ng):
        start = sib * half + chip(dq) * L
        arrived(tok_all.at[rows_at(start, L)], tsem.at[0, 0], tsem.at[3, dq])
        norm_rows(from_ref(tok_all, start), mixg, nrm, start)

    relay(0)
    relay(1)
    whole(0)
    whole(1)
    pad[...] = jnp.zeros_like(pad)
    st[...] = jnp.zeros_like(st)
    taps_n = taps.shape[0]
    reach = taps_n // 2
    lead = (reach + 7) // 8 * 8
    own_cols = p * chans
    eye = lax.broadcasted_iota(jnp.int32, (L, L), 0) == lax.broadcasted_iota(jnp.int32, (L, L), 1)

    def conv_block(b, _):
        rows = rows_at(b * L, L)
        left = nrm[rows, :]
        values = jnp.dot(left, fgv[...], preferred_element_type=F32)
        gating = jnp.dot(left, fgg[...], preferred_element_type=F32)
        glu = (values * jax.nn.sigmoid(gating)).astype(BF16).astype(F32)
        pad[pl.ds(lead, L), :] = glu
        sums = jnp.zeros((L, 1), F32)
        squares = jnp.zeros((L, 1), F32)
        for c in range(chans // 128):
            total = jnp.zeros((L, 128), F32)
            for j in range(taps_n):
                tap = taps[pl.ds(j, 1), rows_at(own_cols + c * 128, 128)]
                total = total + pad[pl.ds(lead - reach + j, L), pl.ds(c * 128, 128)] * tap
            cv[rows, pl.ds(c * 128, 128)] = total
            sums = sums + jnp.sum(total, axis=1, keepdims=True)
            squares = squares + jnp.sum(total * total, axis=1, keepdims=True)
        st[b, pl.ds(0, 1), :] = jnp.sum(jnp.where(eye, sums, 0.0), axis=0, keepdims=True)
        st[b, pl.ds(1, 1), :] = jnp.sum(jnp.where(eye, squares, 0.0), axis=0, keepdims=True)
        return 0

    lax.fori_loop(0, 2 * ng, conv_block, 0)

    slots = [(dq, du) for dq in range(ng) for du in range(2) if (dq, du) != (0, 0)]
    for dq, du in slots:
        push(
            st, st_all.at[dq * 2 + du],
            ssem.at[0, dq * 2 + du], ssem.at[1, dq * 2 + du],
            (fs_of(dq, 0), t if du == 0 else sib),
        )
    forward(3)
    relay(2)
    forward(4)
    for dq, du in slots:
        arrived(st_all.at[dq * 2 + du], ssem.at[0, 0], ssem.at[1, dq * 2 + du])

    def hidden_block(b, _):
        rows = rows_at(b * L, L)
        total = st[b]
        for dq, du in slots:
            total = total + st_all[dq * 2 + du, b]
        count = chans * ng * 2
        sums = jnp.sum(jnp.where(eye, total[0:1, :], 0.0), axis=1, keepdims=True)
        squares = jnp.sum(jnp.where(eye, total[1:2, :], 0.0), axis=1, keepdims=True)
        centre = sums / count
        spread = squares / count - centre * centre
        value = (cv[rows, :] - centre) * lax.rsqrt(spread + norm_floor)
        value = value * chg[:, rows_at(own_cols, chans)]
        hid[rows, :] = (value * jax.nn.sigmoid(value)).astype(BF16)
        return 0

    lax.fori_loop(0, 2 * ng, hidden_block, 0)

    cols = 512

    def reduce_rows(left, right, sbo, sbi, rdo, rdi, k):
        def theirs(n, _):
            at = rows_at(n * cols, cols)
            sbo[:, at] = jnp.dot(
                left[rows_at(sib * half, half), :], right[:, at], preferred_element_type=F32
            ).astype(BF16)
            return 0

        lax.fori_loop(0, width // cols, theirs, 0)
        push(sbo, sbi, rsem.at[k, 0], rsem.at[k, 1], (f, sib))

        def mine(n, _):
            at = rows_at(n * cols, cols)
            acc[:, at] = jnp.dot(
                left[rows_at(t * half, half), :], right[:, at], preferred_element_type=F32
            )
            return 0

        lax.fori_loop(0, width // cols, mine, 0)
        arrived(sbi, rsem.at[k, 0], rsem.at[k, 1])
        for dq in range(1, ng):
            base = chip(dq) * L

            def add(i, _):
                at = pl.ds(pl.multiple_of(base + i * step, step), step)
                rdo[at, :] = (acc[at, :] + sbi[at, :].astype(F32)).astype(BF16)
                return 0

            lax.fori_loop(0, L // step, add, 0)
            push(
                rdo.at[rows_at(base, L)], rdi.at[dq - 1],
                rsem.at[k, 2 * dq], rsem.at[k, 2 * dq + 1], (fs_of(dq, 0), t),
            )

    def reduced(sbi, rdi, i):
        at = pl.ds(pl.multiple_of(p * L + i * step, step), step)
        total = acc[at, :] + sbi[at, :].astype(F32)
        for dq in range(1, ng):
            total = total + rdi[dq - 1, pl.ds(pl.multiple_of(i * step, step), step), :].astype(F32)
        return total.astype(BF16).astype(F32)

    def wait_reduced(rdi, k):
        for dq in range(1, ng):
            arrived(rdi.at[dq - 1], rsem.at[k, 0], rsem.at[k, 2 * dq + 1])

    whole(2)
    reduce_rows(hid, fmo, sbo1, sbi1, rdo1, rdi1, 0)
    wait_reduced(rdi1, 0)

    def resid_rows(i, _):
        at = pl.ds(pl.multiple_of(i * step, step), step)
        own = tok[pl.ds(pl.multiple_of(t * L + i * step, step), step), :].astype(F32)
        value = own + reduced(sbi1, rdi1, i)
        resid[at, :] = value
        scale = lax.rsqrt(jnp.mean(value * value, axis=-1, keepdims=True) + norm_floor)
        nm_all[pl.ds(pl.multiple_of(t * half + p * L + i * step, step), step), :] = (
            value * scale * mlpg[...]
        ).astype(BF16)
        return 0

    lax.fori_loop(0, L // step, resid_rows, 0)
    mine = nm_all.at[rows_at(t * half + p * L, L)]
    for dq in range(1, ng):
        push(mine, mine, nsem.at[0, dq], nsem.at[1, dq], (fs_of(dq, 0), t))
    push(mine, mine, nsem.at[2, 0], nsem.at[3, 0], (f, sib))
    relay(3)
    for dq in range(1, ng):
        block = nm_all.at[rows_at(t * half + chip(dq) * L, L)]
        arrived(block, nsem.at[0, 0], nsem.at[1, dq])
        push(block, block, nsem.at[2, dq], nsem.at[3, dq], (f, sib))

    whole(3)

    def up_half(u):
        def body(n, _):
            at = rows_at(n * 256, 256)
            value = jnp.dot(
                nm_all[rows_at(u * half, half), :], fup[:, at], preferred_element_type=F32
            )
            value = jnp.maximum(value, 0.0)
            act[rows_at(u * half, half), at] = (value * value).astype(BF16)
            return 0

        lax.fori_loop(0, hidden // 256, body, 0)

    up_half(t)
    relay(4, (0, 1))
    for dq in range(ng):
        arrived(nm_all.at[rows_at(sib * half + chip(dq) * L, L)], nsem.at[0, 0], nsem.at[3, dq])
    up_half(sib)
    relay(4, (2, 3))
    whole(4)
    reduce_rows(act, fdn, sbo2, sbi2, rdo2, rdi2, 1)
    wait_reduced(rdi2, 1)

    def finish_rows(i, _):
        at = pl.ds(pl.multiple_of(i * step, step), step)
        value = (resid[at, :] + reduced(sbi2, rdi2, i)).astype(BF16)
        fin[0, at, :] = value
        out[pl.ds(pl.multiple_of(t * L + i * step, step), step), :] = value
        return 0

    lax.fori_loop(0, L // step, finish_rows, 0)
    push(fin.at[0], fin.at[1], fsem.at[0], fsem.at[1], (f, sib))
    arrived(fin.at[1], fsem.at[0], fsem.at[1])

    def copy_rows(i, _):
        at = pl.ds(pl.multiple_of(i * step, step), step)
        out[pl.ds(pl.multiple_of(sib * L + i * step, step), step), :] = fin[1, at, :]
        return 0

    lax.fori_loop(0, L // step, copy_rows, 0)
    for copy in sends:
        copy.wait_send()


def fused_device(ng, nz, tokens, mix_gain, glu_value, glu_gate, conv_taps, chan_gain, mix_out, mlp_gain, up_weight, down_weight):
    rows, width = tokens.shape
    fs = ng * nz
    L = rows // 2
    half = ng * L
    chans = glu_value.shape[1] // ng
    hidden = up_weight.shape[1] // ng
    depth = glu_value.shape[0]
    blocks = 2 * ng
    vm = pltpu.VMEM
    dma = pltpu.SemaphoreType.DMA
    reduce_bufs = [
        vm((half, width), BF16), vm((half, width), BF16), vm((half, width), BF16),
        vm((ng - 1, L, width), BF16),
    ]
    scratch = [
        vm((fs * depth, chans), BF16), vm((fs * depth, chans), BF16), vm((chans, width), BF16),
        vm((fs * depth, hidden), BF16), vm((hidden, width), BF16),
        vm((2 * half, width), BF16), vm((2 * half, width), BF16),
        vm((L + 32, chans), F32), vm((2 * half, chans), F32), vm((2 * half, chans), BF16),
        vm((blocks, 8, L), F32), vm((blocks, blocks, 8, L), F32),
        vm((half, width), F32), vm((L, width), F32), vm((2 * half, width), BF16),
        vm((2 * half, hidden), BF16), vm((2, L, width), BF16),
        *reduce_bufs, *reduce_bufs,
        dma((5, fs)), dma((5, fs)), dma((5,)), dma((4, ng)), dma((4, ng)),
        dma((2, blocks)), dma((2, 2 * ng)), dma((2,)),
    ]
    return pl.pallas_call(
        functools.partial(layer_kernel, ng),
        out_shape=jax.ShapeDtypeStruct((rows, width), BF16),
        in_specs=[pl.BlockSpec(memory_space=vm)] * 10,
        out_specs=pl.BlockSpec(memory_space=vm),
        scratch_shapes=scratch,
        compiler_params=pltpu.CompilerParams(
            collective_id=0, has_side_effects=True, vmem_limit_bytes=60 * 1024 * 1024
        ),
    )(
        tokens, mix_gain[None], glu_value, glu_gate, conv_taps, chan_gain[None], mix_out,
        mlp_gain[None], up_weight, down_weight,
    )


def per_device(*args):
    tokens, glu_value, conv_taps = args[0], args[2], args[4]
    fs, tp = lax.axis_size("fs"), lax.axis_size("tp")
    group = 4
    fits = (
        tp == 2
        and fs == group * 4
        and tokens.shape[0] == 2 * LEN
        and glu_value.shape[0] % 128 == 0
        and conv_taps.shape[1] % (group * 128) == 0
        and conv_taps.shape[0] <= 31
    )
    if fits:
        return fused_device(group, fs // group, *args)
    return plain_device(*args)


def solution(mesh):
    in_specs = (
        P("fs", None),
        P(),
        P("fs", "tp"),
        P("fs", "tp"),
        P(None, "tp"),
        P("tp"),
        P("tp", "fs"),
        P(),
        P("fs", "tp"),
        P("tp", "fs"),
    )
    out_specs = P("fs", None)
    return jax.shard_map(
        per_device, mesh=mesh, in_specs=in_specs, out_specs=out_specs, check_vma=False
    )
```
